256 devices in a mesh: sp: 32 (over z, y), tp: 8 (over x, core).
Axes of the slice: x: 4, y: 4, z: 8, core: 2. Of those that a mesh axis runs over, the one named last changes fastest.
Arguments:
- tokens: bfloat16 [16384, 2048], P(('sp', 'tp')), may hold values from -8 to 8, as said below
- w_query: bfloat16 [2048, 1024], P(None, 'tp'), may hold values from -0.125 to 0.125
- w_key: bfloat16 [2048, 1024], P(None, 'tp'), may hold values from -0.125 to 0.125
- w_value: bfloat16 [2048, 1024], P(None, 'tp'), may hold values from -0.125 to 0.125
- head_bias: float32 [16], P('tp'), may hold values from -40 to -3
- w_out: bfloat16 [1024, 2048], P('tp'), may hold values from -0.1875 to 0.1875
Outputs:
- mixed: bfloat16 [16384, 2048], P(('sp', 'tp'))
The draws below stay inside these ranges and needn't reach their ends.
Inputs may be any that keep to these rules, and one draw needn't show every extreme that they name: `tokens`: activations of order one whose mean shifts between blocks of 512 positions.
All inputs are finite; a program needn't handle non-finite values.
Results may differ from the reference program's by a relative error of at most 0.014.
Values may be sent and summed in bfloat16 or wider, within the bound.
A program may use at most 128 MiB of HBM per device.

```python
import jax
import jax.numpy as jnp
from jax import lax

D = 2048
HEADS = 16
HEAD_DIM = 64
TOK_DEV = 512
TOKENS = 16384
N_SP = 32
N_TP = 8


def draw_tokens(key, part):
    noise = jax.random.normal(jax.random.fold_in(key, 11), (TOKENS, D), jnp.float32)
    spread_level = 1.0
    direction = jax.random.normal(jax.random.fold_in(key, 12), (D,), jnp.float32)
    region_scale = jax.random.uniform(jax.random.fold_in(key, 13), (TOKENS // TOK_DEV,), jnp.float32, -1.2, 1.2)
    level = jnp.repeat(region_scale, TOK_DEV) * spread_level
    values = 0.8 * noise + level[:, None] * direction[None, :]
    return jnp.clip(values, -8.0, 8.0).astype(jnp.bfloat16)


def draw_head_bias(key, part):
    fast_count = HEADS // 2
    ranking = jax.random.permutation(jax.random.fold_in(key, 21), HEADS)
    is_fast = ranking < fast_count
    slow_value = -jnp.log(jnp.float32(TOKENS)) - 1.0 + jax.random.uniform(jax.random.fold_in(key, 22), (HEADS,), jnp.float32, -0.5, 0.5)
    fast_value = -jnp.log(jax.random.uniform(jax.random.fold_in(key, 23), (HEADS,), jnp.float32, 30.0, 100.0)) - 1.0
    return jnp.where(is_fast, fast_value, slow_value).astype(jnp.float32)


def levels(stream_key, extent, split, smallest, largest):
    gain, own = 1.0, jax.random.fold_in(stream_key, 6)
    for dim, shards_of in split:
        draws = jnp.exp(jax.random.uniform(jax.random.fold_in(own, dim), (shards_of,), jnp.float32, smallest / len(split), largest / len(split)))
        gain = gain * jnp.repeat(draws, extent[dim] // shards_of).reshape([-1 if axis == dim else 1 for axis in range(len(extent))])
    return gain


def centred(key, dims, deviation, bound, shards=(), kind=jnp.bfloat16):
    values = deviation * jax.random.normal(key, dims, jnp.float32)
    if shards:
        values = values * levels(key, dims, shards, -0.22, 0.18)
    return jnp.clip(values, -bound, bound).astype(kind)


def setup_inputs(seed: int = 0) -> dict:
    key_of = jax.random.split(jax.random.key(seed), 7)
    tokens = draw_tokens(jax.random.fold_in(key_of[6], 71), 0)
    w_query = centred(key_of[1], (D, HEADS * HEAD_DIM), D ** -0.5, 0.125, ((1, 8),))
    w_key = centred(key_of[2], (D, HEADS * HEAD_DIM), D ** -0.5, 0.125, ((1, 8),))
    w_value = centred(key_of[3], (D, HEADS * HEAD_DIM), D ** -0.5, 0.125, ((1, 8),))
    head_bias = draw_head_bias(jax.random.fold_in(key_of[6], 71), 0)
    w_out = centred(key_of[5], (HEADS * HEAD_DIM, D), (HEADS * HEAD_DIM) ** -0.5, 0.1875, ((0, 8),))
    return dict(tokens=tokens, w_query=w_query, w_key=w_key, w_value=w_value, head_bias=head_bias, w_out=w_out)


def reference(tokens, w_query, w_key, w_value, head_bias, w_out):
    query_all = jnp.dot(tokens, w_query, preferred_element_type=jnp.float32).astype(jnp.bfloat16)
    key_all = jnp.dot(tokens, w_key, preferred_element_type=jnp.float32).astype(jnp.bfloat16)
    value_all = jnp.dot(tokens, w_value, preferred_element_type=jnp.float32).astype(jnp.bfloat16)
    key_pos = jnp.arange(TOKENS, dtype=jnp.int32).reshape(N_SP, TOK_DEV)

    def by_head(head_index):
        first_col = (head_index * HEAD_DIM).astype(jnp.int32)
        query_head = lax.dynamic_slice_in_dim(query_all, first_col, HEAD_DIM, 1)
        key_head = lax.dynamic_slice_in_dim(key_all, first_col, HEAD_DIM, 1)
        value_head = lax.dynamic_slice_in_dim(value_all, first_col, HEAD_DIM, 1)
        value_segments = value_head.reshape(N_SP, TOK_DEV, HEAD_DIM).astype(jnp.float32)
        bias_value = head_bias[head_index]

        def by_block(block_index):
            first_row = (block_index * TOK_DEV).astype(jnp.int32)
            query_block = lax.dynamic_slice_in_dim(query_head, first_row, TOK_DEV, 0)
            query_pos = first_row + jnp.arange(TOK_DEV, dtype=jnp.int32)
            scores = jnp.dot(query_block, key_head.T, preferred_element_type=jnp.float32)
            scores = scores.reshape(TOK_DEV, N_SP, TOK_DEV) * (HEAD_DIM ** -0.5) + bias_value
            causal = key_pos[None] < query_pos[:, None, None]
            log_keep = jnp.where(causal, jax.nn.log_sigmoid(-scores), 0.0)
            tail = lax.cumsum(log_keep, axis=2, reverse=True) - log_keep
            weights = jnp.where(causal, jnp.exp(jax.nn.log_sigmoid(scores) + tail), 0.0).astype(jnp.bfloat16)
            segment_out = jnp.einsum('qst,std->qsd', weights.astype(jnp.float32), value_segments)
            segment_total = jnp.sum(log_keep, axis=2)
            later = lax.cumsum(segment_total, axis=1, reverse=True) - segment_total
            return jnp.sum(jnp.exp(later)[..., None] * segment_out, axis=1)

        return lax.map(by_block, jnp.arange(N_SP, dtype=jnp.int32)).reshape(TOKENS, HEAD_DIM)

    heads_out = lax.map(by_head, jnp.arange(HEADS, dtype=jnp.int32))
    attended = jnp.transpose(heads_out, (1, 0, 2)).reshape(TOKENS, HEADS * HEAD_DIM).astype(jnp.bfloat16)
    group_width = HEADS * HEAD_DIM // N_TP
    total = jnp.zeros((TOKENS, D), jnp.float32)
    for group_index in range(N_TP):
        lower = group_index * group_width
        partial_value = jnp.dot(attended[:, lower:lower + group_width], w_out[lower:lower + group_width, :],
                          preferred_element_type=jnp.float32).astype(jnp.bfloat16)
        partial_value = lax.optimization_barrier(partial_value)
        total = total + partial_value.astype(jnp.float32)
    return total.astype(jnp.bfloat16)
```

```python
import jax, jax.numpy as jnp
from jax import lax
from jax.sharding import PartitionSpec as P
from jax.experimental import pallas as pl
from jax.experimental.pallas import tpu as pltpu

LOG2E = 1.4426950408889634
SEG = 512
N_UNITS = 34
NEG = -1e30

def build_tables(bias2, c, mask_ref, tri_ref):
    rows = lax.broadcasted_iota(jnp.int32, (256, SEG), 0)
    cols = lax.broadcasted_iota(jnp.int32, (256, SEG), 1)
    qpos = (2 * (rows // 64) + c) * 64 + rows % 64
    mask_ref[0] = jnp.full((256, SEG), bias2, jnp.float32)
    mask_ref[1] = jnp.where(cols < qpos, bias2, NEG)
    mask_ref[2] = jnp.full((256, SEG), NEG, jnp.float32)
    j = lax.broadcasted_iota(jnp.int32, (SEG, SEG), 0)
    s = lax.broadcasted_iota(jnp.int32, (SEG, SEG), 1)
    tri_ref[...] = jnp.where(j > s, -1.0, 0.0).astype(jnp.bfloat16)

def attend(z, q_ref, kv_ref, mask_ref, tri_ref, sp_ref, ls_ref, w_ref, f_ref, acc_ref, RC=128):
    n_a = 4 * z + 2
    zm = 7 - z

    def place(n):
        is_b = (n >= n_a).astype(jnp.int32)
        s = n - is_b * n_a
        first = is_b * (4 * zm + 2) + (1 - is_b) * (4 * z)
        return is_b, s, first

    def stage1(n):
        is_b, s, first = place(n)
        slot = n % 2
        kv = kv_ref[s]
        for r in range(0, 512, RC):
            half = r // 256
            b = first + half
            idx = (s >= b).astype(jnp.int32) + (s > b).astype(jnp.int32)
            q = q_ref[pl.ds(pl.multiple_of(is_b * 512, 512) + r, RC), :]
            sc = lax.dot_general(q, kv, (((1,), (1,)), ((), ())), preferred_element_type=jnp.float32)
            sc = sc + mask_ref[idx, pl.ds(r % 256, RC), :]
            l = jnp.log2(1.0 + jnp.exp2(jnp.minimum(sc, 126.0)))
            sp = jnp.maximum(l, sc)
            sp_ref[slot, pl.ds(r, RC), :] = sp.astype(jnp.bfloat16)
            ls_ref[slot, pl.ds(r, RC), :] = sc - sp

    def stage2(n):
        slot = n % 2
        for r in range(0, 512, RC):
            sp = sp_ref[slot, pl.ds(r, RC), :]
            lo = jnp.dot(sp, tri_ref[:, 0:256], preferred_element_type=jnp.float32)
            hi = jnp.dot(sp[:, 256:], tri_ref[256:, 256:], preferred_element_type=jnp.float32)
            w_ref[slot, pl.ds(r, RC), 0:256] = jnp.exp2(ls_ref[slot, pl.ds(r, RC), 0:256] + lo).astype(jnp.bfloat16)
            w_ref[slot, pl.ds(r, RC), 256:512] = jnp.exp2(ls_ref[slot, pl.ds(r, RC), 256:512] + hi).astype(jnp.bfloat16)
            keep = lo[:, 0:1] - sp[:, 0:1].astype(jnp.float32)
            f_ref[slot, pl.ds(r, RC), :] = jnp.exp2(jnp.broadcast_to(keep, (RC, 128)))

    def stage3(n):
        is_b, s, _ = place(n)
        slot = n % 2
        kv = kv_ref[s]
        for r in range(0, 512, RC):
            rows = pl.ds(pl.multiple_of(is_b * 512, 512) + r, RC)
            pv = jnp.dot(w_ref[slot, pl.ds(r, RC), :], kv, preferred_element_type=jnp.float32)
            acc_ref[rows, :] = acc_ref[rows, :] * f_ref[slot, pl.ds(r, RC), :] + pv

    acc_ref[...] = jnp.zeros_like(acc_ref)
    stage1(0)
    stage2(0)
    stage1(1)

    def body(i, carry):
        stage3(i)
        stage2(i + 1)
        stage1(i + 2)
        return carry

    lax.fori_loop(0, N_UNITS - 2, body, 0)
    stage3(N_UNITS - 2)
    stage2(N_UNITS - 1)
    stage3(N_UNITS - 1)

SCRATCH = lambda: [
    pltpu.VMEM((3, 256, SEG), jnp.float32),
    pltpu.VMEM((SEG, SEG), jnp.bfloat16),
    pltpu.VMEM((2, 512, SEG), jnp.bfloat16),
    pltpu.VMEM((2, 512, SEG), jnp.float32),
    pltpu.VMEM((2, 512, SEG), jnp.bfloat16),
    pltpu.VMEM((2, 512, 128), jnp.float32),
    pltpu.VMEM((1024, 128), jnp.float32),
]


def kernel(b_ref, q_ref, kv_ref, o_ref, mask_ref, tri_ref, sp_ref, ls_ref, w_ref, f_ref, acc_ref):
    z = lax.axis_index("sp") // 4
    c = lax.axis_index("tp") % 2
    build_tables(b_ref[0] * LOG2E, c, mask_ref, tri_ref)
    attend(z, q_ref, kv_ref, mask_ref, tri_ref, sp_ref, ls_ref, w_ref, f_ref, acc_ref)
    o_ref[...] = acc_ref[...].astype(jnp.bfloat16)


def shards(tokens, w_query, w_key, w_value, head_bias, w_out):
    same_core = [[0, 2, 4, 6], [1, 3, 5, 7]]
    pair = [[0, 1], [2, 3], [4, 5], [6, 7]]
    along_y = [[4 * z + y for y in range(4)] for z in range(8)]
    along_z = [[4 * z + y for z in range(8)] for y in range(4)]
    mirror = [(4 * z + y, 4 * (7 - z) + y) for z in range(8) for y in range(4)]
    y = lax.axis_index("sp") % 4
    rows = lax.all_gather(tokens, "tp", axis_index_groups=same_core, axis=0, tiled=True)
    own = jnp.concatenate([w_query.reshape(-1, 2, 64), w_key.reshape(-1, 2, 64), w_value.reshape(-1, 2, 64)], axis=2)
    both = lax.all_gather(own, "tp", axis_index_groups=pair, axis=1, tiled=True)
    bias = lax.all_gather(head_bias, "tp", axis_index_groups=pair, axis=0, tiled=True)
    full_out = lax.all_gather(w_out, "tp", axis=0, tiled=True)
    qkv = jnp.dot(rows, both.reshape(-1, 768), preferred_element_type=jnp.float32).reshape(256, 4, 192)
    scale = jnp.where(jnp.arange(192) < 64, LOG2E / 8, 1.0)
    qkv = jnp.moveaxis((qkv * scale).astype(jnp.bfloat16), 1, 0)
    qkv = lax.all_to_all(qkv, "sp", 0, 0, axis_index_groups=along_y, tiled=True)
    q, kv = qkv[..., :64], qkv[..., 64:]
    away = lax.ppermute(q[2:], "sp", mirror)
    q = jnp.concatenate([q[:2], away], axis=0).reshape(1024, 64)
    q = jnp.pad(q, ((0, 0), (0, 64)))
    kv = lax.all_gather(kv, "sp", axis_index_groups=along_z, axis=0, tiled=True)
    kv = lax.all_gather(kv.reshape(32, 4, 64, 128), "tp", axis_index_groups=pair, axis=0)
    kv = jnp.moveaxis(kv, 0, 2).reshape(32, 512, 128)
    out = pl.pallas_call(
        kernel,
        out_shape=jax.ShapeDtypeStruct((1024, 128), jnp.bfloat16),
        in_specs=[pl.BlockSpec(memory_space=pltpu.SMEM)] + [pl.BlockSpec(memory_space=pltpu.VMEM)] * 2,
        out_specs=pl.BlockSpec(memory_space=pltpu.VMEM),
        scratch_shapes=SCRATCH(),
        compiler_params=pltpu.CompilerParams(vmem_limit_bytes=48 * 2**20),
        cost_estimate=pl.CostEstimate(flops=40 * 10**9, bytes_accessed=5 * 10**6, transcendentals=0),
        name="attn",
    )(lax.dynamic_slice_in_dim(bias, y, 1), q, kv)
    out = out[:, 64:].reshape(4, 4, 64, 64)
    out = jnp.concatenate([out[:2], lax.ppermute(out[2:], "sp", mirror)], axis=0)
    out = lax.all_to_all(out, "sp", 0, 0, axis_index_groups=along_y, tiled=True)
    out = lax.all_to_all(out, "tp", 1, 1, axis_index_groups=same_core, tiled=True)
    out = jnp.transpose(out, (2, 1, 0, 3)).reshape(64, 1024)
    return jnp.dot(out, full_out, preferred_element_type=jnp.float32).astype(jnp.bfloat16)


def solution(mesh):
    placed = (P(("sp", "tp"), None), P(None, "tp"), P(None, "tp"), P(None, "tp"), P("tp"), P("tp", None))
    return jax.shard_map(
        shards, mesh=mesh, in_specs=placed, out_specs=P(("sp", "tp"), None), check_vma=False
    )
```

```python
import jax, jax.numpy as jnp
from jax import lax
from jax.sharding import PartitionSpec as P
from jax.experimental import pallas as pl
from jax.experimental.pallas import tpu as pltpu

LOG2E = 1.4426950408889634
SEG = 512
N_UNITS = 34
NEG = -1e30

def build_tables(bias2, c, mask_ref, tri_ref):
    rows = lax.broadcasted_iota(jnp.int32, (256, SEG), 0)
    cols = lax.broadcasted_iota(jnp.int32, (256, SEG), 1)
    qpos = (2 * (rows // 64) + c) * 64 + rows % 64
    mask_ref[0] = jnp.full((256, SEG), bias2, jnp.float32)
    mask_ref[1] = jnp.where(cols < qpos, bias2, NEG)
    mask_ref[2] = jnp.full((256, SEG), NEG, jnp.float32)
    j = lax.broadcasted_iota(jnp.int32, (SEG, SEG), 0)
    s = lax.broadcasted_iota(jnp.int32, (SEG, SEG), 1)
    tri_ref[...] = jnp.where(j > s, -1.0, 0.0).astype(jnp.bfloat16)

def attend(z, q_ref, kv_ref, mask_ref, tri_ref, sp_ref, ls_ref, w_ref, f_ref, acc_ref, RC=128):
    n_a = 4 * z + 2
    zm = 7 - z

    def place(n):
        is_b = (n >= n_a).astype(jnp.int32)
        s = n - is_b * n_a
        first = is_b * (4 * zm + 2) + (1 - is_b) * (4 * z)
        return is_b, s, first

    def stage1(n):
        is_b, s, first = place(n)
        slot = n % 2
        kv = kv_ref[s].reshape(SEG, 128)
        for r in range(0, 512, RC):
            half = r // 256
            b = first + half
            idx = (s >= b).astype(jnp.int32) + (s > b).astype(jnp.int32)
            q = q_ref[pl.ds(pl.multiple_of(is_b * 512, 512) + r, RC), :]
            sc = lax.dot_general(q, kv, (((1,), (1,)), ((), ())), preferred_element_type=jnp.float32)
            sc = sc + mask_ref[idx, pl.ds(r % 256, RC), :]
            l = jnp.log2(1.0 + jnp.exp2(jnp.minimum(sc, 126.0)))
            sp = jnp.maximum(l, sc)
            sp_ref[slot, pl.ds(r, RC), :] = sp.astype(jnp.bfloat16)
            ls_ref[slot, pl.ds(r, RC), :] = sc - sp

    def stage2(n):
        slot = n % 2
        for r in range(0, 512, RC):
            sp = sp_ref[slot, pl.ds(r, RC), :]
            lo = jnp.dot(sp, tri_ref[:, 0:256], preferred_element_type=jnp.float32)
            hi = jnp.dot(sp[:, 256:], tri_ref[256:, 256:], preferred_element_type=jnp.float32)
            w_ref[slot, pl.ds(r, RC), 0:256] = jnp.exp2(ls_ref[slot, pl.ds(r, RC), 0:256] + lo).astype(jnp.bfloat16)
            w_ref[slot, pl.ds(r, RC), 256:512] = jnp.exp2(ls_ref[slot, pl.ds(r, RC), 256:512] + hi).astype(jnp.bfloat16)
            keep = lo[:, 0:1] - sp[:, 0:1].astype(jnp.float32)
            f_ref[slot, pl.ds(r, RC), :] = jnp.exp2(jnp.broadcast_to(keep, (RC, 128)))

    def stage3(n):
        is_b, s, _ = place(n)
        slot = n % 2
        kv = kv_ref[s].reshape(SEG, 128)
        for r in range(0, 512, RC):
            rows = pl.ds(pl.multiple_of(is_b * 512, 512) + r, RC)
            pv = jnp.dot(w_ref[slot, pl.ds(r, RC), :], kv, preferred_element_type=jnp.float32)
            acc_ref[rows, :] = acc_ref[rows, :] * f_ref[slot, pl.ds(r, RC), :] + pv

    stage1(0)
    stage2(0)
    stage1(1)

    def body(i, carry):
        stage3(i)
        stage2(i + 1)
        stage1(i + 2)
        return carry

    lax.fori_loop(0, N_UNITS - 2, body, 0)
    stage3(N_UNITS - 2)
    stage2(N_UNITS - 1)
    stage3(N_UNITS - 1)


MESH = pl.DeviceIdType.MESH


def kernel(
    tok_hbm, wq_hbm, wk_hbm, wv_hbm, bias_hbm, wo_hbm, o_ref,
    tok, wq, wk, wv, bias, wo, qs, kvs, qp, q, kv, ob, at,
    mask_ref, tri_ref, sp_ref, ls_ref, w_ref, f_ref, acc_ref,
    loc, tok_s, tok_r, w_s, w_r, wo_s, wo_r, wos_s, wos_r,
    q_s, q_r, ya_s, ya_r, zr_s, zr_r, zl_s, zl_r, sib_s, sib_r, ex_s, ex_r,
):
    sp, tp = lax.axis_index("sp"), lax.axis_index("tp")
    z, y, x, c = sp // 4, sp % 4, tp // 2, tp % 2
    zm = 7 - z

    def dev(xx, yy, zz, cc):
        return (4 * zz + yy, 2 * xx + cc)

    def remote(src, dst, s, r, to):
        return pltpu.make_async_remote_copy(
            src_ref=src, dst_ref=dst, send_sem=s, recv_sem=r, device_id=to, device_id_type=MESH
        )

    sib = dev(x, y, z, 1 - c)
    right, left = dev(x, y, (z + 1) % 8, c), dev(x, y, (z + 7) % 8, c)

    locals_ = [
        pltpu.make_async_copy(a, b, loc.at[i])
        for i, (a, b) in enumerate(
            [(tok_hbm, tok.at[x]), (wq_hbm, wq.at[c]), (wk_hbm, wk.at[c]), (wv_hbm, wv.at[c]),
             (bias_hbm, bias.at[c]), (wo_hbm, wo.at[tp])]
        )
    ]
    for cp in locals_:
        cp.start()

    barrier = pltpu.get_barrier_semaphore()
    for dx in range(4):
        for dy in range(4):
            if dx or dy:
                pl.semaphore_signal(barrier, inc=1, device_id=dev((x + dx) % 4, (y + dy) % 4, z, c), device_id_type=MESH)
            pl.semaphore_signal(barrier, inc=1, device_id=dev((x + dx) % 4, (y + dy) % 4, zm, c), device_id_type=MESH)
    for to in (sib, right, left):
        pl.semaphore_signal(barrier, inc=1, device_id=to, device_id_type=MESH)
    pl.semaphore_wait(barrier, 34)

    sends = []
    for d in (1, 3, 2):
        cp = remote(tok_hbm, tok.at[x], tok_s.at[d], tok_r.at[x], dev((x + d) % 4, y, z, c))
        cp.start()
        sends.append(cp)
    for i, (a, b) in enumerate([(wq_hbm, wq), (wk_hbm, wk), (wv_hbm, wv), (bias_hbm, bias)]):
        cp = remote(a, b.at[c], w_s.at[i], w_r.at[i], sib)
        cp.start()
        sends.append(cp)
    for i, (a, b) in enumerate([(wq_hbm, wq), (wk_hbm, wk), (wv_hbm, wv), (bias_hbm, bias)]):
        remote(a, b.at[1 - c], w_s.at[i], w_r.at[i], sib).wait_recv()
    for cp in locals_:
        cp.wait()

    b2 = bias[y // 2, pl.ds(y % 2, 1), :][:, 0:1] * LOG2E
    build_tables(b2, c, mask_ref, tri_ref)
    acc_ref[...] = jnp.zeros_like(acc_ref)

    for d in (1, 3, 2):
        xs = (x + d) % 4
        remote(tok_hbm, tok.at[xs], tok_s.at[d], tok_r.at[xs], sib).wait_recv()

    for d in (1, 3, 2):
        cp = remote(wo_hbm, wo.at[tp], wo_s.at[d], wo_r.at[x], dev((x + d) % 4, y, z, c))
        cp.start()
        sends.append(cp)

    rows = tok[...].reshape(256, 2048)
    for cc in range(2):
        qq = jnp.dot(rows, wq[cc], preferred_element_type=jnp.float32) * (LOG2E / 8)
        kk = jnp.dot(rows, wk[cc], preferred_element_type=jnp.float32)
        vv = jnp.dot(rows, wv[cc], preferred_element_type=jnp.float32)
        for j in range(2):
            lanes = slice(64 * j, 64 * j + 64)
            both = jnp.concatenate([vv[:, lanes], kk[:, lanes]], axis=1).astype(jnp.bfloat16)
            kvs[2 * cc + j] = both.reshape(4, 64, 128)
            packed = jnp.concatenate([qq[:128, lanes], qq[128:, lanes]], axis=1)
            qs[2 * cc + j] = packed.astype(jnp.bfloat16)

    for d in (1, 3, 2):
        yp = (y + d) % 4
        cp = remote(kvs.at[yp], kv.at[4 * z + y, :, c], ya_s.at[d], ya_r.at[y], dev(x, yp, z, c))
        cp.start()
        sends.append(cp)
    own = pltpu.make_async_copy(kvs.at[y], kv.at[4 * z + y, :, c], loc.at[6])
    own.start()
    zq = jnp.where(y < 2, z, zm)
    for d in (1, 3, 2):
        yp = (y + d) % 4
        cp = remote(qs.at[yp], qp.at[y], q_s.at[d], q_r.at[y], dev(x, yp, zq, c))
        cp.start()
        sends.append(cp)

    @pl.when(y < 2)
    def _():
        cp = pltpu.make_async_copy(qs.at[y], qp.at[y], loc.at[7])
        cp.start()
        cp.wait()

    @pl.when(y >= 2)
    def _():
        remote(qs.at[y], qp.at[y], q_s.at[0], q_r.at[y], dev(x, y, zm, c)).start()

    own.wait()

    def piece(zz, j):
        return kv.at[4 * zz + j, :, c]

    def pass_on(zz, j):
        cp = remote(piece(zz, j), piece(zz, j), sib_s.at[4 * zz + j], sib_r.at[4 * zz + j], sib)
        cp.start()
        sends.append(cp)

    def hop(way, t, j):
        zz = (z + 8 - t) % 8 if way == 0 else (z + t) % 8
        s, r = ((zr_s, zr_r), (zl_s, zl_r))[way]
        return remote(piece(zz, j), piece(zz, j), s.at[4 * t + j], r.at[4 * t + j], (right, left)[way])

    def landed(way, t, j):
        zz = (z + 8 - t) % 8 if way == 0 else (z + t) % 8
        s, r = ((zr_s, zr_r), (zl_s, zl_r))[way]
        remote(piece(zz, j), piece(zz, j), s.at[4 * t - 4 + j], r.at[4 * t - 4 + j], (right, left)[way]).wait_recv()
        return zz

    for j in range(4):
        @pl.when(y != j)
        def _():
            remote(kvs.at[0], piece(z, j), ya_s.at[1], ya_r.at[j], sib).wait_recv()
        for way in range(2):
            cp = hop(way, 0, j)
            cp.start()
            sends.append(cp)
        pass_on(z, j)
    for t in range(1, 5):
        for j in range(4):
            for way in range(2):
                if t < 4 or way == j // 2:
                    zz = landed(way, t, j)
                    if t < 3 or (t == 3 and way == j // 2):
                        cp = hop(way, t, j)
                        cp.start()
                        sends.append(cp)
                    pass_on(zz, j)

    for j in range(4):
        @pl.when((y != j) | (y >= 2))
        def _():
            remote(qs.at[0], qp.at[j], q_s.at[0], q_r.at[j], sib).wait_recv()
        low = qp[j].astype(jnp.float32)
        nil = jnp.zeros((128, 64), jnp.float32)
        q[pl.ds(256 * j, 128), :] = jnp.concatenate([nil, low[:, :64]], axis=1).astype(jnp.bfloat16)
        q[pl.ds(256 * j + 128, 128), :] = jnp.concatenate([nil, low[:, 64:]], axis=1).astype(jnp.bfloat16)

    for d in (1, 3, 2):
        xs = (x + d) % 4
        remote(wo_hbm, wo.at[2 * xs + c], wo_s.at[d], wo_r.at[xs], sib).wait_recv()
    for xs in range(4):
        cp = remote(wo.at[2 * xs + c], wo.at[2 * xs + c], wos_s.at[xs], wos_r.at[xs], sib)
        cp.start()
        sends.append(cp)

    for zz in range(8):
        for j in range(4):
            there = kv.at[4 * zz + j, :, 1 - c]
            remote(there, there, sib_s.at[4 * zz + j], sib_r.at[4 * zz + j], sib).wait_recv()

    attend(z, q, kv, mask_ref, tri_ref, sp_ref, ls_ref, w_ref, f_ref, acc_ref)

    ob[...] = acc_ref[...].astype(jnp.bfloat16)
    hh = 4 * x + y
    for i in range(4):
        for d in range(4):
            xb = (x + d) % 4
            src = ob.at[pl.ds(256 * i + pl.multiple_of(64 * xb, 64), 64), :]
            cp = remote(src, at.at[hh], ex_s.at[4 * i + d], ex_r.at[hh], dev(xb, i, z if i < 2 else zm, c))
            if d == 0 and i < 2:
                @pl.when(y != i)
                def _():
                    cp.start()

                @pl.when(y == i)
                def _():
                    here = pltpu.make_async_copy(src, at.at[hh], loc.at[8])
                    here.start()
                    here.wait()
            else:
                cp.start()
                sends.append(cp)
    for xs in range(4):
        there = wo.at[2 * xs + 1 - c]
        remote(there, there, wos_s.at[xs], wos_r.at[xs], sib).wait_recv()
    for g in range(16):
        @pl.when((hh != g) | (y >= 2))
        def _():
            remote(ob.at[pl.ds(0, 64), :], at.at[g], ex_s.at[0], ex_r.at[g], sib).wait_recv()

    pairs = [
        jnp.concatenate([at[2 * p].astype(jnp.float32)[:, :64], at[2 * p + 1].astype(jnp.float32)[:, :64]], axis=1).astype(jnp.bfloat16)
        for p in range(8)
    ]
    every = jnp.concatenate(pairs, axis=1)
    for n in range(0, 2048, 512):
        o_ref[:, n : n + 512] = jnp.dot(
            every, wo[:, :, n : n + 512].reshape(1024, 512), preferred_element_type=jnp.float32
        ).astype(jnp.bfloat16)

    for cp in sends:
        cp.wait_send()

    @pl.when(y >= 2)
    def _():
        remote(qs.at[y], qp.at[y], q_s.at[0], q_r.at[y], dev(x, y, zm, c)).wait_send()

    for i in range(2):
        @pl.when(y != i)
        def _():
            remote(ob.at[pl.ds(0, 64), :], at.at[hh], ex_s.at[4 * i], ex_r.at[hh], sib).wait_send()


def shards(tokens, w_query, w_key, w_value, head_bias, w_out):
    bf, f32 = jnp.bfloat16, jnp.float32
    dma = pltpu.SemaphoreType.DMA
    return pl.pallas_call(
        kernel,
        out_shape=jax.ShapeDtypeStruct((64, 2048), bf),
        in_specs=[pl.BlockSpec(memory_space=pl.ANY)] * 6,
        out_specs=pl.BlockSpec(memory_space=pltpu.VMEM),
        scratch_shapes=[
            pltpu.VMEM((4, 64, 2048), bf),
            pltpu.VMEM((2, 2048, 128), bf),
            pltpu.VMEM((2, 2048, 128), bf),
            pltpu.VMEM((2, 2048, 128), bf),
            pltpu.VMEM((2, 8, 128), f32),
            pltpu.VMEM((8, 128, 2048), bf),
            pltpu.VMEM((4, 128, 128), bf),
            pltpu.VMEM((4, 4, 64, 128), bf),
            pltpu.VMEM((4, 128, 128), bf),
            pltpu.VMEM((1024, 128), bf),
            pltpu.VMEM((32, 4, 2, 64, 128), bf),
            pltpu.VMEM((1024, 128), bf),
            pltpu.VMEM((16, 64, 128), bf),
            pltpu.VMEM((3, 256, SEG), f32),
            pltpu.VMEM((SEG, SEG), bf),
            pltpu.VMEM((2, SEG, SEG), bf),
            pltpu.VMEM((2, SEG, SEG), f32),
            pltpu.VMEM((2, SEG, SEG), bf),
            pltpu.VMEM((2, SEG, 128), f32),
            pltpu.VMEM((1024, 128), f32),
            dma((9,)), dma((4,)), dma((4,)), dma((4,)), dma((4,)), dma((4,)), dma((4,)), dma((4,)), dma((4,)),
            dma((4,)), dma((4,)), dma((4,)), dma((4,)), dma((16,)), dma((16,)), dma((16,)), dma((16,)),
            dma((32,)), dma((32,)), dma((16,)), dma((16,)),
        ],
        compiler_params=pltpu.CompilerParams(
            vmem_limit_bytes=60 * 2**20, collective_id=0, has_side_effects=True
        ),
        name="layer",
    )(tokens, w_query, w_key, w_value, jnp.broadcast_to(jnp.pad(head_bias, (0, 6))[:, None], (8, 128)), w_out)


def solution(mesh):
    placed = (P(("sp", "tp"), None), P(None, "tp"), P(None, "tp"), P(None, "tp"), P("tp"), P("tp", None))
    return jax.shard_map(
        shards, mesh=mesh, in_specs=placed, out_specs=P(("sp", "tp"), None), check_vma=False
    )
```

```python
import jax, jax.numpy as jnp
from jax import lax
from jax.sharding import PartitionSpec as P
from jax.experimental import pallas as pl
from jax.experimental.pallas import tpu as pltpu

LOG2E = 1.4426950408889634
SEG = 512
N_UNITS = 34
WO_ON, WO_SHARE = 14, 24
ORDER = (0, 7, 1, 6, 2, 5, 3, 4)
NEG = -1e30

def build_tables(bias2, c, mask_ref, tri_ref):
    rows = lax.broadcasted_iota(jnp.int32, (256, SEG), 0)
    cols = lax.broadcasted_iota(jnp.int32, (256, SEG), 1)
    qpos = (2 * (rows // 64) + c) * 64 + rows % 64
    mask_ref[0] = jnp.full((256, SEG), bias2, jnp.float32)
    mask_ref[1] = jnp.where(cols < qpos, bias2, NEG)
    mask_ref[2] = jnp.full((256, SEG), NEG, jnp.float32)
    j = lax.broadcasted_iota(jnp.int32, (SEG, SEG), 0)
    s = lax.broadcasted_iota(jnp.int32, (SEG, SEG), 1)
    tri_ref[...] = jnp.where(j > s, -1.0, 0.0).astype(jnp.bfloat16)

def attend(z, arrive, take_q, q_ref, kv_ref, mask_ref, tri_ref, sp_ref, ls_ref, w_ref, f_ref, acc_ref, fac_ref, RC=128):
    zm = 7 - z
    parts = []
    start = 0
    for k in range(8):
        zz = (z + ORDER[k]) % 8
        a = 4 * (zz < z).astype(jnp.int32) + 2 * (zz == z).astype(jnp.int32)
        parts.append((start, zz, a))
        start = start + a + 4 * (zz <= zm).astype(jnp.int32)

    def place(n):
        base, zz, a = parts[0]
        step = 0
        for k in range(1, 8):
            at_k = n >= parts[k][0]
            base = jnp.where(at_k, parts[k][0], base)
            zz = jnp.where(at_k, parts[k][1], zz)
            a = jnp.where(at_k, parts[k][2], a)
            step = jnp.where(at_k, (k + 1) // 2, step)
        i = n - base
        is_b = (i >= a).astype(jnp.int32)
        s = 4 * zz + i - is_b * a
        first = is_b * (4 * zm + 2) + (1 - is_b) * (4 * z)
        return (is_b, s, first, is_b * 8 + zz), step

    def stage1(n, unit):
        is_b, s, first, _ = unit
        slot = n % 2
        kv = kv_ref[s].reshape(SEG, 128)
        for r in range(0, 512, RC):
            b = first + r // 256
            idx = (s >= b).astype(jnp.int32) + (s > b).astype(jnp.int32)
            q = q_ref[pl.ds(pl.multiple_of(is_b * 512, 512) + r, RC), :]
            sc = lax.dot_general(q, kv, (((1,), (1,)), ((), ())), preferred_element_type=jnp.float32)
            sc = sc + mask_ref[idx, pl.ds(r % 256, RC), :]
            l = jnp.log2(1.0 + jnp.exp2(jnp.minimum(sc, 126.0)))
            sp = jnp.maximum(l, sc)
            sp_ref[slot, pl.ds(r, RC), :] = sp.astype(jnp.bfloat16)
            ls_ref[slot, pl.ds(r, RC), :] = sc - sp

    def stage2(n):
        slot = n % 2
        for r in range(0, 512, RC):
            sp = sp_ref[slot, pl.ds(r, RC), :]
            lo = jnp.dot(sp, tri_ref[:, 0:256], preferred_element_type=jnp.float32)
            hi = jnp.dot(sp[:, 256:], tri_ref[256:, 256:], preferred_element_type=jnp.float32)
            w_ref[slot, pl.ds(r, RC), 0:256] = jnp.exp2(ls_ref[slot, pl.ds(r, RC), 0:256] + lo).astype(jnp.bfloat16)
            w_ref[slot, pl.ds(r, RC), 256:512] = jnp.exp2(ls_ref[slot, pl.ds(r, RC), 256:512] + hi).astype(jnp.bfloat16)
            keep = lo[:, 0:1] - sp[:, 0:1].astype(jnp.float32)
            f_ref[slot, pl.ds(r, RC), :] = jnp.exp2(jnp.broadcast_to(keep, (RC, 128)))

    def stage3(n, unit):
        _, s, _, at = unit
        slot = n % 2
        kv = kv_ref[s].reshape(SEG, 128)
        for r in range(0, 512, RC):
            rows = pl.ds(r, RC)
            pv = jnp.dot(w_ref[slot, rows, :], kv, preferred_element_type=jnp.float32)
            f = f_ref[slot, rows, :]
            acc_ref[at, rows, :] = acc_ref[at, rows, :] * f + pv
            fac_ref[at, rows, :] = fac_ref[at, rows, :] * f

    u0, _ = place(0)
    u1, step = place(1)
    done, sib_done = arrive(1, step, 6, 0)
    stage1(0, u0)
    stage2(0)
    stage1(1, u1)
    take_q(2)
    take_q(3)

    def body(i, carry):
        done, sib_done, ua, ub = carry
        uc, step = place(i + 2)
        done, sib_done = arrive(i + 2, step, done, sib_done)
        stage3(i, ua)
        stage2(i + 1)
        stage1(i + 2, uc)
        return done, sib_done, ub, uc

    done, sib_done, ua, ub = lax.fori_loop(0, N_UNITS - 2, body, (done, sib_done, u0, u1))
    arrive(N_UNITS, 4, done, sib_done)
    stage3(N_UNITS - 2, ua)
    stage2(N_UNITS - 1)
    stage3(N_UNITS - 1, ub)


MESH = pl.DeviceIdType.MESH


def kernel(
    tok_hbm, wq_hbm, wk_hbm, wv_hbm, bias_hbm, wo_hbm, o_ref,
    tok, wq, wk, wv, bias, wo, qs, kvs, qp, q, kv, ob, at,
    mask_ref, tri_ref, sp_ref, ls_ref, w_ref, f_ref, acc_ref, fac_ref,
    loc, own_s, ownq_s, tok_s, tok_r, w_s, w_r, wo_s, wo_r, wos_s, wos_r,
    q_s, q_r, ya_s, ya_r, zr_s, zr_r, zl_s, zl_r, sib_s, sib_r, ex_s, ex_r,
):
    sp, tp = lax.axis_index("sp"), lax.axis_index("tp")
    z, y, x, c = sp // 4, sp % 4, tp // 2, tp % 2
    zm = 7 - z

    def dev(xx, yy, zz, cc):
        return (4 * zz + yy, 2 * xx + cc)

    def remote(src, dst, s, r, to):
        return pltpu.make_async_remote_copy(
            src_ref=src, dst_ref=dst, send_sem=s, recv_sem=r, device_id=to, device_id_type=MESH
        )

    sib = dev(x, y, z, 1 - c)
    right, left = dev(x, y, (z + 1) % 8, c), dev(x, y, (z + 7) % 8, c)

    locals_ = [
        pltpu.make_async_copy(a, b, loc.at[i])
        for i, (a, b) in enumerate(
            [(tok_hbm, tok.at[x]), (wq_hbm, wq.at[c]), (wk_hbm, wk.at[c]), (wv_hbm, wv.at[c]),
             (bias_hbm, bias.at[c]), (wo_hbm, wo.at[tp])]
        )
    ]
    for cp in locals_:
        cp.start()

    barrier = pltpu.get_barrier_semaphore()
    for dx in range(4):
        for dy in range(4):
            if dx or dy:
                pl.semaphore_signal(barrier, inc=1, device_id=dev((x + dx) % 4, (y + dy) % 4, z, c), device_id_type=MESH)
            pl.semaphore_signal(barrier, inc=1, device_id=dev((x + dx) % 4, (y + dy) % 4, zm, c), device_id_type=MESH)
    for to in (sib, right, left):
        pl.semaphore_signal(barrier, inc=1, device_id=to, device_id_type=MESH)
    pl.semaphore_wait(barrier, 34)

    x_right, x_left = dev((x + 1) % 4, y, z, c), dev((x + 3) % 4, y, z, c)
    around = (x, (x + 3) % 4, (x + 1) % 4, (x + 2) % 4)
    halves = (pl.ds(0, 32), pl.ds(32, 32))
    sends = []

    def go(cp):
        cp.start()
        sends.append(cp)

    for i in range(2):
        go(remote(tok_hbm.at[halves[i]], tok.at[x, halves[i]], tok_s.at[i], tok_r.at[2 + i], x_right))
        go(remote(tok_hbm.at[halves[1 - i]], tok.at[x, halves[1 - i]], tok_s.at[3 - i], tok_r.at[5 - i], x_left))
    shared = [(wq_hbm, wq), (wk_hbm, wk), (wv_hbm, wv), (bias_hbm, bias)]
    for i, (a, b) in enumerate(shared):
        go(remote(a, b.at[c], w_s.at[i], w_r.at[i], sib))

    acc_ref[...] = jnp.zeros_like(acc_ref)
    fac_ref[...] = jnp.ones_like(fac_ref)
    for i, (a, b) in enumerate(shared):
        remote(a, b.at[1 - c], w_s.at[i], w_r.at[i], sib).wait_recv()
    for cp in locals_:
        cp.wait()

    def tok_landed(o, i):
        there = tok.at[around[o], halves[i]]
        remote(there, there, tok_s.at[0], tok_r.at[2 * o + i], sib).wait_recv()

    def tok_on(o, i):
        there = tok.at[around[o], halves[i]]
        go(remote(there, there, tok_s.at[3 + o], tok_r.at[6 + i], x_right if o == 1 else x_left))

    zq = jnp.where(y < 2, z, zm)

    def own_q(o):
        xb = around[o]

        @pl.when(y < 2)
        def _():
            pltpu.make_async_copy(qs.at[y, xb], qp.at[y, xb], ownq_s.at[o]).start()

        @pl.when(y >= 2)
        def _():
            remote(qs.at[y, xb], qp.at[y, xb], q_s.at[4 * o], q_r.at[4 * y + o], dev(x, y, zm, c)).start()

    def project(o):
        xb = around[o]
        rows = tok[xb]
        for cc in range(2):
            qq = jnp.dot(rows, wq[cc], preferred_element_type=jnp.float32) * (LOG2E / 8)
            kk = jnp.dot(rows, wk[cc], preferred_element_type=jnp.float32)
            vv = jnp.dot(rows, wv[cc], preferred_element_type=jnp.float32)
            for j in range(2):
                lanes = slice(64 * j, 64 * j + 64)
                kvs[2 * cc + j, xb] = jnp.concatenate([vv[:, lanes], kk[:, lanes]], axis=1).astype(jnp.bfloat16)
                qs[2 * cc + j, xb] = jnp.concatenate([qq[:32, lanes], qq[32:, lanes]], axis=1).astype(jnp.bfloat16)
        for d in (1, 3, 2):
            yp = (y + d) % 4
            go(remote(qs.at[yp, xb], qp.at[y, xb], q_s.at[4 * o + d], q_r.at[4 * y + o], dev(x, yp, zq, c)))
        own_q(o)
        for d in (1, 3, 2):
            yp = (y + d) % 4
            go(remote(kvs.at[yp, xb], kv.at[4 * z + y, xb, c], ya_s.at[4 * o + d], ya_r.at[4 * o + y], dev(x, yp, z, c)))
        pltpu.make_async_copy(kvs.at[y, xb], kv.at[4 * z + y, xb, c], own_s.at[o]).start()

    def piece(zz, o):
        return kv.at[pl.ds(4 * zz, 4), row_of(o), c]

    def row_of(o):
        if isinstance(o, int):
            return around[o]
        return (x + jnp.where(o == 0, 0, jnp.where(o == 1, 3, o - 1))) % 4

    def pass_on(zz, o):
        return remote(piece(zz, o), piece(zz, o), sib_s.at[4 * zz + o], sib_r.at[4 * zz + o], sib)

    def source(way, t):
        return (z + 8 - t) % 8 if way == 0 else (z + t) % 8

    def hop(way, t, o, landing=0):
        zz = source(way, t + landing)
        s, r = ((zr_s, zr_r), (zl_s, zl_r))[way]
        return remote(piece(zz, o), piece(zz, o), s.at[4 * t + o], r.at[4 * t + o], (right, left)[way])

    def start_z(o):
        for d in (1, 3, 2):
            ys = (y + d) % 4
            there = kv.at[4 * z + ys, around[o], c]
            remote(there, there, ya_s.at[0], ya_r.at[4 * o + ys], sib).wait_recv()
        pltpu.make_async_copy(kvs.at[y, around[o]], kv.at[4 * z + y, around[o], c], own_s.at[o]).wait()
        for way in range(2):
            go(hop(way, 0, o))
        go(pass_on(z, o))

    project(0)
    tok_landed(1, 0)
    tok_on(1, 0)
    tok_landed(2, 1)
    tok_on(2, 1)
    both = bias[y // 2]
    b2 = jnp.where(y % 2 == 0, both[:, 0:1], both[:, 1:2]) * LOG2E
    start_z(0)
    tok_landed(1, 1)
    project(1)
    tok_landed(2, 0)
    project(2)
    start_z(1)
    tok_landed(3, 0)
    tok_landed(3, 1)
    project(3)
    go(remote(wo_hbm, wo.at[tp], wo_s.at[0], wo_r.at[2], x_right))
    go(remote(wo_hbm, wo.at[tp], wo_s.at[1], wo_r.at[4], x_left))
    build_tables(b2, c, mask_ref, tri_ref)
    def take_q(j):
        @pl.when((y == j) & (y < 2))
        def _():
            for o in range(4):
                pltpu.make_async_copy(qs.at[y, 0], qp.at[y, 0], ownq_s.at[o]).wait()

        @pl.when((y != j) | (y >= 2))
        def _():
            for o in range(4):
                remote(qs.at[0, 0], qp.at[j, around[o]], q_s.at[0], q_r.at[4 * j + o], sib).wait_recv()
        for xb in range(4):
            low = qp[j, xb].astype(jnp.float32)
            nil = jnp.zeros((32, 64), jnp.float32)
            at_row = 256 * j + 64 * xb
            q[pl.ds(at_row, 32), :] = jnp.concatenate([nil, low[:, :64]], axis=1).astype(jnp.bfloat16)
            q[pl.ds(at_row + 32, 32), :] = jnp.concatenate([nil, low[:, 64:]], axis=1).astype(jnp.bfloat16)

    wo_half = (pl.ds(0, 64), pl.ds(64, 64))

    def wo_hop(o, i):
        there = wo.at[2 * around[o] + c, wo_half[i]]
        return remote(there, there, wo_s.at[1 + o], wo_r.at[6 + i], x_right if o == 1 else x_left)

    def wo_share(o):
        there = wo.at[2 * around[o] + c]
        return remote(there, there, wos_s.at[o], wos_r.at[o], sib)

    def event(e, carry):
        t, o = e // 4, e % 4
        for way in range(2):
            @pl.when((t < 4) | (o // 2 == way))
            def _():
                hop(way, t - 1, o, 1).wait_recv()

                @pl.when((t < 3) | ((t == 3) & (o // 2 == way)))
                def _():
                    hop(way, t, o).start()
                pass_on(source(way, t), o).start()
        return carry

    def sib_event(e, carry):
        t, o = e // 4, e % 4

        def wait_for(zz):
            there = kv.at[pl.ds(4 * zz, 4), row_of(o), 1 - c]
            remote(there, there, sib_s.at[0], sib_r.at[4 * zz + o], sib).wait_recv()

        wait_for(source(0, t))

        @pl.when((t > 0) & (t < 4))
        def _():
            wait_for(source(1, t))
        return carry

    start_z(2)
    event(4, 0)
    take_q(0)
    take_q(1)
    start_z(3)
    event(5, 0)

    def arrive(n, step, done, sib_done):
        need = 4 * step + 4
        upto = jnp.maximum(need, jnp.minimum(20, 6 + n * 2 // 3))
        lax.fori_loop(done, upto, event, 0)
        done = jnp.maximum(done, upto)
        lax.fori_loop(sib_done, need, sib_event, 0)
        sib_done = jnp.maximum(sib_done, need)

        @pl.when(n == WO_ON)
        def _():
            for o in (1, 2):
                there = wo.at[2 * around[o] + c]
                remote(there, there, wo_s.at[0], wo_r.at[2 * o], sib).wait_recv()
                wo_hop(o, o - 1).start()

        @pl.when(n == WO_SHARE)
        def _():
            for i in range(2):
                there = wo.at[2 * around[3] + c, wo_half[i]]
                remote(there, there, wo_s.at[0], wo_r.at[6 + i], sib).wait_recv()
            for o in range(4):
                wo_share(o).start()
        return done, sib_done

    attend(z, arrive, take_q, q, kv, mask_ref, tri_ref, sp_ref, ls_ref, w_ref, f_ref, acc_ref, fac_ref)

    for b in range(2):
        for r in range(0, 512, 64):
            rows = pl.ds(r, 64)
            total = acc_ref[8 * b, rows, :]
            for zz in range(1, 8):
                total = total * fac_ref[8 * b + zz, rows, :] + acc_ref[8 * b + zz, rows, :]
            ob[pl.ds(512 * b + r, 64), :] = total.astype(jnp.bfloat16)
    hh = 4 * x + y
    for i in range(4):
        for d in range(4):
            xb = (x + d) % 4
            src = ob.at[pl.ds(256 * i + pl.multiple_of(64 * xb, 64), 64), :]
            cp = remote(src, at.at[hh], ex_s.at[4 * i + d], ex_r.at[hh], dev(xb, i, z if i < 2 else zm, c))
            if d == 0 and i < 2:
                @pl.when(y != i)
                def _():
                    cp.start()

                @pl.when(y == i)
                def _():
                    here = pltpu.make_async_copy(src, at.at[hh], loc.at[8])
                    here.start()
                    here.wait()
            else:
                cp.start()
                sends.append(cp)
    for o in range(4):
        there = wo.at[2 * around[o] + 1 - c]
        remote(there, there, wos_s.at[o], wos_r.at[o], sib).wait_recv()
    for g in range(16):
        @pl.when((hh != g) | (y >= 2))
        def _():
            remote(ob.at[pl.ds(0, 64), :], at.at[g], ex_s.at[0], ex_r.at[g], sib).wait_recv()

    pairs = [
        jnp.concatenate([at[2 * p].astype(jnp.float32)[:, :64], at[2 * p + 1].astype(jnp.float32)[:, :64]], axis=1).astype(jnp.bfloat16)
        for p in range(8)
    ]
    every = jnp.concatenate(pairs, axis=1)
    for n in range(0, 2048, 512):
        o_ref[:, n : n + 512] = jnp.dot(
            every, wo[:, :, n : n + 512].reshape(1024, 512), preferred_element_type=jnp.float32
        ).astype(jnp.bfloat16)

    for cp in sends:
        cp.wait_send()
    for o in range(4):
        wo_share(o).wait_send()
    for o in (1, 2):
        wo_hop(o, o - 1).wait_send()
    for t in range(1, 5):
        for o in range(4):
            for way in range(2):
                if t < 4 or o // 2 == way:
                    if t < 3 or (t == 3 and o // 2 == way):
                        hop(way, t, o).wait_send()
                    pass_on(source(way, t), o).wait_send()

    @pl.when(y >= 2)
    def _():
        for o in range(4):
            remote(qs.at[y, 0], qp.at[y, 0], q_s.at[4 * o], q_r.at[0], dev(x, y, zm, c)).wait_send()

    for i in range(2):
        @pl.when(y != i)
        def _():
            remote(ob.at[pl.ds(0, 64), :], at.at[hh], ex_s.at[4 * i], ex_r.at[hh], sib).wait_send()


def shards(tokens, w_query, w_key, w_value, head_bias, w_out):
    bf, f32 = jnp.bfloat16, jnp.float32
    dma = pltpu.SemaphoreType.DMA
    return pl.pallas_call(
        kernel,
        out_shape=jax.ShapeDtypeStruct((64, 2048), bf),
        in_specs=[pl.BlockSpec(memory_space=pl.ANY)] * 6,
        out_specs=pl.BlockSpec(memory_space=pltpu.VMEM),
        scratch_shapes=[
            pltpu.VMEM((4, 64, 2048), bf),
            pltpu.VMEM((2, 2048, 128), bf),
            pltpu.VMEM((2, 2048, 128), bf),
            pltpu.VMEM((2, 2048, 128), bf),
            pltpu.VMEM((2, 1, 2), f32),
            pltpu.VMEM((8, 128, 2048), bf),
            pltpu.VMEM((4, 4, 32, 128), bf),
            pltpu.VMEM((4, 4, 64, 128), bf),
            pltpu.VMEM((4, 4, 32, 128), bf),
            pltpu.VMEM((1024, 128), bf),
            pltpu.VMEM((32, 4, 2, 64, 128), bf),
            pltpu.VMEM((1024, 128), bf),
            pltpu.VMEM((16, 64, 128), bf),
            pltpu.VMEM((3, 256, SEG), f32),
            pltpu.VMEM((SEG, SEG), bf),
            pltpu.VMEM((2, SEG, SEG), bf),
            pltpu.VMEM((2, SEG, SEG), f32),
            pltpu.VMEM((2, SEG, SEG), bf),
            pltpu.VMEM((2, SEG, 128), f32),
            pltpu.VMEM((16, SEG, 128), f32),
            pltpu.VMEM((16, SEG, 128), f32),
            dma((9,)), dma((4,)), dma((4,)), dma((6,)), dma((8,)), dma((4,)), dma((4,)), dma((4,)), dma((8,)), dma((4,)),
            dma((4,)), dma((16,)), dma((16,)), dma((16,)), dma((16,)), dma((16,)), dma((16,)), dma((16,)), dma((16,)),
            dma((32,)), dma((32,)), dma((16,)), dma((16,)),
        ],
        compiler_params=pltpu.CompilerParams(
            vmem_limit_bytes=60 * 2**20, collective_id=0, has_side_effects=True
        ),
        name="layer",
    )(tokens, w_query, w_key, w_value, head_bias.reshape(1, 2), w_out)


def solution(mesh):
    placed = (P(("sp", "tp"), None), P(None, "tp"), P(None, "tp"), P(None, "tp"), P("tp"), P("tp", None))
    return jax.shard_map(
        shards, mesh=mesh, in_specs=placed, out_specs=P(("sp", "tp"), None), check_vma=False
    )
```

```python
import jax, jax.numpy as jnp
from jax import lax
from jax.sharding import PartitionSpec as P
from jax.experimental import pallas as pl
from jax.experimental.pallas import tpu as pltpu

LOG2E = 1.4426950408889634
SEG = 512
N_UNITS = 34
WO_ON, WO_SHARE = 6, 11
ORDER = (0, 7, 1, 6, 2, 5, 3, 4)
NEG = -1e30

def build_tables(bias2, c, mask_ref, tri_ref):
    rows = lax.broadcasted_iota(jnp.int32, (256, SEG), 0)
    cols = lax.broadcasted_iota(jnp.int32, (256, SEG), 1)
    qpos = (2 * (rows // 64) + c) * 64 + rows % 64
    mask_ref[0] = jnp.full((256, SEG), bias2, jnp.float32)
    mask_ref[1] = jnp.where(cols < qpos, bias2, NEG)
    mask_ref[2] = jnp.full((256, SEG), NEG, jnp.float32)
    j = lax.broadcasted_iota(jnp.int32, (SEG, SEG), 0)
    s = lax.broadcasted_iota(jnp.int32, (SEG, SEG), 1)
    tri_ref[...] = jnp.where(j > s, -1.0, 0.0).astype(jnp.bfloat16)

def attend(z, arrive, take_q, q_ref, kv_ref, mask_ref, tri_ref, sp_ref, ls_ref, w_ref, f_ref, acc_ref, fac_ref, RC=128):
    zm = 7 - z
    parts = []
    start = 0
    for k in range(8):
        zz = (z + ORDER[k]) % 8
        a = 4 * (zz < z).astype(jnp.int32) + 2 * (zz == z).astype(jnp.int32)
        b = 4 * (zz <= zm).astype(jnp.int32)
        parts.append((start, zz, a if k == 0 else 0, b))
        start = start + a + b

    def place(n):
        base, zz, lo, b = parts[0]
        step = 0
        for k in range(1, 8):
            at_k = n >= parts[k][0]
            base = jnp.where(at_k, parts[k][0], base)
            zz = jnp.where(at_k, parts[k][1], zz)
            lo = jnp.where(at_k, parts[k][2], lo)
            b = jnp.where(at_k, parts[k][3], b)
            step = jnp.where(at_k, (k + 1) // 2, step)
        i = n - base
        is_b = ((i >= lo) & (i < lo + b)).astype(jnp.int32)
        s = 4 * zz + i - jnp.where(is_b == 1, lo, jnp.where(i < lo, 0, b))
        first = is_b * (4 * zm + 2) + (1 - is_b) * (4 * z)
        return (is_b, s, first, is_b * 8 + zz), step

    def stage1(slot, unit):
        is_b, s, first, _ = unit
        kv = kv_ref[s].reshape(SEG, 128)
        for r in range(0, 512, RC):
            b = first + r // 256
            idx = (s >= b).astype(jnp.int32) + (s > b).astype(jnp.int32)
            q = q_ref[pl.ds(pl.multiple_of(is_b * 512, 512) + r, RC), :]
            sc = lax.dot_general(q, kv, (((1,), (1,)), ((), ())), preferred_element_type=jnp.float32)
            sc = sc + mask_ref[idx, pl.ds(r % 256, RC), :]
            l = jnp.log2(1.0 + jnp.exp2(jnp.minimum(sc, 126.0)))
            sp = jnp.maximum(l, sc)
            sp_ref[slot, pl.ds(r, RC), :] = sp.astype(jnp.bfloat16)
            ls_ref[slot, pl.ds(r, RC), :] = sc - sp

    def stage2(slot):
        for r in range(0, 512, RC):
            sp = sp_ref[slot, pl.ds(r, RC), :]
            lo = jnp.dot(sp, tri_ref[:, 0:256], preferred_element_type=jnp.float32)
            hi = jnp.dot(sp[:, 256:], tri_ref[256:, 256:], preferred_element_type=jnp.float32)
            w_ref[slot, pl.ds(r, RC), 0:256] = jnp.exp2(ls_ref[slot, pl.ds(r, RC), 0:256] + lo).astype(jnp.bfloat16)
            w_ref[slot, pl.ds(r, RC), 256:512] = jnp.exp2(ls_ref[slot, pl.ds(r, RC), 256:512] + hi).astype(jnp.bfloat16)
            keep = lo[:, 0:1] - sp[:, 0:1].astype(jnp.float32)
            f_ref[slot, pl.ds(r, RC), :] = jnp.exp2(jnp.broadcast_to(keep, (RC, 128)))

    def stage3(slot, unit):
        _, s, _, at = unit
        kv = kv_ref[s].reshape(SEG, 128)
        for r in range(0, 512, RC):
            rows = pl.ds(r, RC)
            pv = jnp.dot(w_ref[slot, rows, :], kv, preferred_element_type=jnp.float32)
            f = f_ref[slot, rows, :]
            acc_ref[at, rows, :] = acc_ref[at, rows, :] * f + pv
            fac_ref[at, rows, :] = fac_ref[at, rows, :] * f

    u0, _ = place(0)
    u1, step = place(1)
    done, sib_done = arrive(-1, step, 7, 0)
    stage1(0, u0)
    stage2(0)
    stage1(1, u1)
    take_q(2)
    take_q(3)

    def body(i, carry):
        done, sib_done, ua, ub = carry
        uc, _ = place(2 * i + 2)
        ud, step = place(2 * i + 3)
        done, sib_done = arrive(i, step, done, sib_done)
        stage3(0, ua)
        stage2(1)
        stage1(0, uc)
        stage3(1, ub)
        stage2(0)
        stage1(1, ud)
        return done, sib_done, uc, ud

    done, sib_done, ua, ub = lax.fori_loop(0, (N_UNITS - 2) // 2, body, (done, sib_done, u0, u1))
    arrive(N_UNITS, 4, done, sib_done)
    stage3(0, ua)
    stage2(1)
    stage3(1, ub)


MESH = pl.DeviceIdType.MESH


def kernel(
    tok_hbm, wq_hbm, wk_hbm, wv_hbm, bias_hbm, wo_hbm, o_ref,
    tok, wq, wk, wv, bias, wo, qs, kvs, qp, q, kv, ob, at,
    mask_ref, tri_ref, sp_ref, ls_ref, w_ref, f_ref, acc_ref, fac_ref,
    loc, own_s, ownq_s, tok_s, tok_r, w_s, w_r, wo_s, wo_r, wos_s, wos_r,
    q_s, q_r, ya_s, ya_r, zr_s, zr_r, zl_s, zl_r, sib_s, sib_r, ex_s, ex_r,
):
    sp, tp = lax.axis_index("sp"), lax.axis_index("tp")
    z, y, x, c = sp // 4, sp % 4, tp // 2, tp % 2
    zm = 7 - z

    def dev(xx, yy, zz, cc):
        return (4 * zz + yy, 2 * xx + cc)

    def remote(src, dst, s, r, to):
        return pltpu.make_async_remote_copy(
            src_ref=src, dst_ref=dst, send_sem=s, recv_sem=r, device_id=to, device_id_type=MESH
        )

    sib = dev(x, y, z, 1 - c)
    right, left = dev(x, y, (z + 1) % 8, c), dev(x, y, (z + 7) % 8, c)

    locals_ = [
        pltpu.make_async_copy(a, b, loc.at[i])
        for i, (a, b) in enumerate(
            [(tok_hbm, tok.at[x]), (wq_hbm, wq.at[c]), (wk_hbm, wk.at[c]), (wv_hbm, wv.at[c]),
             (bias_hbm, bias.at[c]), (wo_hbm, wo.at[tp])]
        )
    ]
    for cp in locals_:
        cp.start()

    barrier = pltpu.get_barrier_semaphore()
    for dx in range(4):
        for dy in range(4):
            if dx or dy:
                pl.semaphore_signal(barrier, inc=1, device_id=dev((x + dx) % 4, (y + dy) % 4, z, c), device_id_type=MESH)
            pl.semaphore_signal(barrier, inc=1, device_id=dev((x + dx) % 4, (y + dy) % 4, zm, c), device_id_type=MESH)
    for to in (sib, right, left):
        pl.semaphore_signal(barrier, inc=1, device_id=to, device_id_type=MESH)
    pl.semaphore_wait(barrier, 34)

    x_right, x_left = dev((x + 1) % 4, y, z, c), dev((x + 3) % 4, y, z, c)
    around = (x, (x + 3) % 4, (x + 1) % 4, (x + 2) % 4)
    halves = (pl.ds(0, 32), pl.ds(32, 32))
    sends = []

    def go(cp):
        cp.start()
        sends.append(cp)

    for i in range(2):
        go(remote(tok_hbm.at[halves[i]], tok.at[x, halves[i]], tok_s.at[i], tok_r.at[2 + i], x_right))
        go(remote(tok_hbm.at[halves[1 - i]], tok.at[x, halves[1 - i]], tok_s.at[3 - i], tok_r.at[5 - i], x_left))
    shared = [(wq_hbm, wq), (wk_hbm, wk), (wv_hbm, wv), (bias_hbm, bias)]
    for i, (a, b) in enumerate(shared):
        go(remote(a, b.at[c], w_s.at[i], w_r.at[i], sib))

    acc_ref[...] = jnp.zeros_like(acc_ref)
    fac_ref[...] = jnp.ones_like(fac_ref)
    for i, (a, b) in enumerate(shared):
        remote(a, b.at[1 - c], w_s.at[i], w_r.at[i], sib).wait_recv()
    for cp in locals_:
        cp.wait()

    def tok_landed(o, i):
        there = tok.at[around[o], halves[i]]
        remote(there, there, tok_s.at[0], tok_r.at[2 * o + i], sib).wait_recv()

    def tok_on(o, i):
        there = tok.at[around[o], halves[i]]
        go(remote(there, there, tok_s.at[3 + o], tok_r.at[6 + i], x_right if o == 1 else x_left))

    zq = jnp.where(y < 2, z, zm)

    def own_q(o):
        xb = around[o]

        @pl.when(y < 2)
        def _():
            pltpu.make_async_copy(qs.at[y, xb], qp.at[y, xb], ownq_s.at[o]).start()

        @pl.when(y >= 2)
        def _():
            remote(qs.at[y, xb], qp.at[y, xb], q_s.at[4 * o], q_r.at[4 * y + o], dev(x, y, zm, c)).start()

    def project(o):
        xb = around[o]
        rows = tok[xb]
        for cc in range(2):
            qq = jnp.dot(rows, wq[cc], preferred_element_type=jnp.float32) * (LOG2E / 8)
            kk = jnp.dot(rows, wk[cc], preferred_element_type=jnp.float32)
            vv = jnp.dot(rows, wv[cc], preferred_element_type=jnp.float32)
            for j in range(2):
                lanes = slice(64 * j, 64 * j + 64)
                kvs[2 * cc + j, xb] = jnp.concatenate([vv[:, lanes], kk[:, lanes]], axis=1).astype(jnp.bfloat16)
                qs[2 * cc + j, xb] = jnp.concatenate([qq[:32, lanes], qq[32:, lanes]], axis=1).astype(jnp.bfloat16)
        for d in (1, 3, 2):
            yp = (y + d) % 4
            go(remote(qs.at[yp, xb], qp.at[y, xb], q_s.at[4 * o + d], q_r.at[4 * y + o], dev(x, yp, zq, c)))
        own_q(o)
        for d in (1, 3, 2):
            yp = (y + d) % 4
            go(remote(kvs.at[yp, xb], kv.at[4 * z + y, xb, c], ya_s.at[4 * o + d], ya_r.at[4 * o + y], dev(x, yp, z, c)))
        pltpu.make_async_copy(kvs.at[y, xb], kv.at[4 * z + y, xb, c], own_s.at[o]).start()

    def piece(zz, o):
        return kv.at[pl.ds(4 * zz, 4), row_of(o), c]

    def row_of(o):
        if isinstance(o, int):
            return around[o]
        return (x + jnp.where(o == 0, 0, jnp.where(o == 1, 3, o - 1))) % 4

    def pass_on(zz, o):
        return remote(piece(zz, o), piece(zz, o), sib_s.at[4 * zz + o], sib_r.at[4 * zz + o], sib)

    def source(way, t):
        return (z + 8 - t) % 8 if way == 0 else (z + t) % 8

    def hop(way, t, o, landing=0):
        zz = source(way, t + landing)
        s, r = ((zr_s, zr_r), (zl_s, zl_r))[way]
        return remote(piece(zz, o), piece(zz, o), s.at[4 * t + o], r.at[4 * t + o], (right, left)[way])

    def start_z(o):
        for d in (1, 3, 2):
            ys = (y + d) % 4
            there = kv.at[4 * z + ys, around[o], c]
            remote(there, there, ya_s.at[0], ya_r.at[4 * o + ys], sib).wait_recv()
        pltpu.make_async_copy(kvs.at[y, around[o]], kv.at[4 * z + y, around[o], c], own_s.at[o]).wait()
        for way in range(2):
            go(hop(way, 0, o))
        go(pass_on(z, o))

    project(0)
    tok_landed(1, 0)
    tok_on(1, 0)
    tok_landed(2, 1)
    tok_on(2, 1)
    both = bias[y // 2]
    b2 = jnp.where(y % 2 == 0, both[:, 0:1], both[:, 1:2]) * LOG2E
    start_z(0)
    tok_landed(1, 1)
    project(1)
    tok_landed(2, 0)
    project(2)
    start_z(1)
    tok_landed(3, 0)
    tok_landed(3, 1)
    project(3)
    go(remote(wo_hbm, wo.at[tp], wo_s.at[0], wo_r.at[2], x_right))
    go(remote(wo_hbm, wo.at[tp], wo_s.at[1], wo_r.at[4], x_left))
    build_tables(b2, c, mask_ref, tri_ref)
    def take_q(j):
        @pl.when((y == j) & (y < 2))
        def _():
            for o in range(4):
                pltpu.make_async_copy(qs.at[y, 0], qp.at[y, 0], ownq_s.at[o]).wait()

        @pl.when((y != j) | (y >= 2))
        def _():
            for o in range(4):
                remote(qs.at[0, 0], qp.at[j, around[o]], q_s.at[0], q_r.at[4 * j + o], sib).wait_recv()
        for xb in range(4):
            low = qp[j, xb].astype(jnp.float32)
            nil = jnp.zeros((32, 64), jnp.float32)
            at_row = 256 * j + 64 * xb
            q[pl.ds(at_row, 32), :] = jnp.concatenate([nil, low[:, :64]], axis=1).astype(jnp.bfloat16)
            q[pl.ds(at_row + 32, 32), :] = jnp.concatenate([nil, low[:, 64:]], axis=1).astype(jnp.bfloat16)

    wo_half = (pl.ds(0, 64), pl.ds(64, 64))

    def wo_hop(o, i):
        there = wo.at[2 * around[o] + c, wo_half[i]]
        return remote(there, there, wo_s.at[1 + o], wo_r.at[6 + i], x_right if o == 1 else x_left)

    def wo_share(o):
        there = wo.at[2 * around[o] + c]
        return remote(there, there, wos_s.at[o], wos_r.at[o], sib)

    def event(e, carry):
        t, o = e // 4, e % 4
        for way in range(2):
            @pl.when((t < 4) | (o // 2 == way))
            def _():
                hop(way, t - 1, o, 1).wait_recv()

                @pl.when((t < 3) | ((t == 3) & (o // 2 == way)))
                def _():
                    hop(way, t, o).start()
                pass_on(source(way, t), o).start()
        return carry

    def sib_event(e, carry):
        t, o = e // 4, e % 4

        def wait_for(zz):
            there = kv.at[pl.ds(4 * zz, 4), row_of(o), 1 - c]
            remote(there, there, sib_s.at[0], sib_r.at[4 * zz + o], sib).wait_recv()

        wait_for(source(0, t))

        @pl.when((t > 0) & (t < 4))
        def _():
            wait_for(source(1, t))
        return carry

    start_z(2)
    event(4, 0)
    take_q(0)
    take_q(1)
    start_z(3)
    event(5, 0)
    event(6, 0)

    def arrive(n, step, done, sib_done):
        need = 4 * step + 4
        upto = jnp.maximum(need, jnp.minimum(20, 9 + n * 4 // 3))
        lax.fori_loop(done, upto, event, 0)
        done = jnp.maximum(done, upto)
        lax.fori_loop(sib_done, need, sib_event, 0)
        sib_done = jnp.maximum(sib_done, need)

        @pl.when(n == WO_ON)
        def _():
            for o in (1, 2):
                there = wo.at[2 * around[o] + c]
                remote(there, there, wo_s.at[0], wo_r.at[2 * o], sib).wait_recv()
                wo_hop(o, o - 1).start()

        @pl.when(n == WO_SHARE)
        def _():
            for i in range(2):
                there = wo.at[2 * around[3] + c, wo_half[i]]
                remote(there, there, wo_s.at[0], wo_r.at[6 + i], sib).wait_recv()
            for o in range(4):
                wo_share(o).start()
        return done, sib_done

    attend(z, arrive, take_q, q, kv, mask_ref, tri_ref, sp_ref, ls_ref, w_ref, f_ref, acc_ref, fac_ref)

    for b in range(2):
        for r in range(0, 512, 64):
            rows = pl.ds(r, 64)
            total = acc_ref[8 * b, rows, :]
            for zz in range(1, 8):
                total = total * fac_ref[8 * b + zz, rows, :] + acc_ref[8 * b + zz, rows, :]
            ob[pl.ds(256 * b + r // 2, 32), :] = jnp.concatenate([total[:32, :64], total[32:, :64]], axis=1).astype(
                jnp.bfloat16
            )
    hh = 4 * x + y
    for i in range(4):
        for d in range(4):
            xb = (x + d) % 4
            src = ob.at[pl.ds(128 * i + pl.multiple_of(32 * xb, 32), 32), :]
            cp = remote(src, at.at[hh], ex_s.at[4 * i + d], ex_r.at[hh], dev(xb, i, z if i < 2 else zm, c))
            if d == 0 and i < 2:
                @pl.when(y != i)
                def _():
                    cp.start()

                @pl.when(y == i)
                def _():
                    here = pltpu.make_async_copy(src, at.at[hh], loc.at[8])
                    here.start()
                    here.wait()
            else:
                cp.start()
                sends.append(cp)
    for o in range(4):
        there = wo.at[2 * around[o] + 1 - c]
        remote(there, there, wos_s.at[o], wos_r.at[o], sib).wait_recv()
    for g in range(16):
        @pl.when((hh != g) | (y >= 2))
        def _():
            remote(ob.at[pl.ds(0, 32), :], at.at[g], ex_s.at[0], ex_r.at[g], sib).wait_recv()

    heads = [at[h].astype(jnp.float32) for h in range(16)]
    upper = jnp.concatenate([head[:, :64] for head in heads], axis=1)
    lower = jnp.concatenate([head[:, 64:] for head in heads], axis=1)
    every = jnp.concatenate([upper, lower], axis=0).astype(jnp.bfloat16)
    for n in range(0, 2048, 512):
        o_ref[:, n : n + 512] = jnp.dot(
            every, wo[:, :, n : n + 512].reshape(1024, 512), preferred_element_type=jnp.float32
        ).astype(jnp.bfloat16)

    for cp in sends:
        cp.wait_send()
    for o in range(4):
        wo_share(o).wait_send()
    for o in (1, 2):
        wo_hop(o, o - 1).wait_send()
    for t in range(1, 5):
        for o in range(4):
            for way in range(2):
                if t < 4 or o // 2 == way:
                    if t < 3 or (t == 3 and o // 2 == way):
                        hop(way, t, o).wait_send()
                    pass_on(source(way, t), o).wait_send()

    @pl.when(y >= 2)
    def _():
        for o in range(4):
            remote(qs.at[y, 0], qp.at[y, 0], q_s.at[4 * o], q_r.at[0], dev(x, y, zm, c)).wait_send()

    for i in range(2):
        @pl.when(y != i)
        def _():
            remote(ob.at[pl.ds(0, 32), :], at.at[hh], ex_s.at[4 * i], ex_r.at[hh], sib).wait_send()


def shards(tokens, w_query, w_key, w_value, head_bias, w_out):
    bf, f32 = jnp.bfloat16, jnp.float32
    dma = pltpu.SemaphoreType.DMA
    return pl.pallas_call(
        kernel,
        out_shape=jax.ShapeDtypeStruct((64, 2048), bf),
        in_specs=[pl.BlockSpec(memory_space=pl.ANY)] * 6,
        out_specs=pl.BlockSpec(memory_space=pltpu.VMEM),
        scratch_shapes=[
            pltpu.VMEM((4, 64, 2048), bf),
            pltpu.VMEM((2, 2048, 128), bf),
            pltpu.VMEM((2, 2048, 128), bf),
            pltpu.VMEM((2, 2048, 128), bf),
            pltpu.VMEM((2, 1, 2), f32),
            pltpu.VMEM((8, 128, 2048), bf),
            pltpu.VMEM((4, 4, 32, 128), bf),
            pltpu.VMEM((4, 4, 64, 128), bf),
            pltpu.VMEM((4, 4, 32, 128), bf),
            pltpu.VMEM((1024, 128), bf),
            pltpu.VMEM((32, 4, 2, 64, 128), bf),
            pltpu.VMEM((512, 128), bf),
            pltpu.VMEM((16, 32, 128), bf),
            pltpu.VMEM((3, 256, SEG), f32),
            pltpu.VMEM((SEG, SEG), bf),
            pltpu.VMEM((2, SEG, SEG), bf),
            pltpu.VMEM((2, SEG, SEG), f32),
            pltpu.VMEM((2, SEG, SEG), bf),
            pltpu.VMEM((2, SEG, 128), f32),
            pltpu.VMEM((16, SEG, 128), f32),
            pltpu.VMEM((16, SEG, 128), f32),
            dma((9,)), dma((4,)), dma((4,)), dma((6,)), dma((8,)), dma((4,)), dma((4,)), dma((4,)), dma((8,)), dma((4,)),
            dma((4,)), dma((16,)), dma((16,)), dma((16,)), dma((16,)), dma((16,)), dma((16,)), dma((16,)), dma((16,)),
            dma((32,)), dma((32,)), dma((16,)), dma((16,)),
        ],
        compiler_params=pltpu.CompilerParams(
            vmem_limit_bytes=60 * 2**20, collective_id=0, has_side_effects=True
        ),
        name="layer",
    )(tokens, w_query, w_key, w_value, head_bias.reshape(1, 2), w_out)


def solution(mesh):
    placed = (P(("sp", "tp"), None), P(None, "tp"), P(None, "tp"), P(None, "tp"), P("tp"), P("tp", None))
    return jax.shard_map(
        shards, mesh=mesh, in_specs=placed, out_specs=P(("sp", "tp"), None), check_vma=False
    )
```

```python
import jax, jax.numpy as jnp
from jax import lax
from jax.sharding import PartitionSpec as P
from jax.experimental import pallas as pl
from jax.experimental.pallas import tpu as pltpu

LOG2E = 1.4426950408889634
SEG = 512
N_UNITS = 34
WO_ON, WO_SHARE = 8, 13
ORDER = (0, 7, 1, 6, 2, 5, 3, 4)
NEG = -1e30

def build_tables(bias2, c, mask_ref, tri_ref):
    rows = lax.broadcasted_iota(jnp.int32, (256, SEG), 0)
    cols = lax.broadcasted_iota(jnp.int32, (256, SEG), 1)
    qpos = (2 * (rows // 64) + c) * 64 + rows % 64
    mask_ref[0] = jnp.full((256, SEG), bias2, jnp.float32)
    mask_ref[1] = jnp.where(cols < qpos, bias2, NEG)
    mask_ref[2] = jnp.full((256, SEG), NEG, jnp.float32)
    j = lax.broadcasted_iota(jnp.int32, (SEG, SEG), 0)
    s = lax.broadcasted_iota(jnp.int32, (SEG, SEG), 1)
    tri_ref[...] = jnp.where(j > s, -1.0, 0.0).astype(jnp.bfloat16)

def attend(z, arrive, take_q, q_ref, kv_ref, mask_ref, tri_ref, sp_ref, ls_ref, w_ref, f_ref, acc_ref, fac_ref, RC=128):
    zm = 7 - z
    parts = []
    start = 0
    for k in range(8):
        zz = (z + ORDER[k]) % 8
        a = 4 * (zz < z).astype(jnp.int32) + 2 * (zz == z).astype(jnp.int32)
        b = 4 * (zz <= zm).astype(jnp.int32)
        parts.append((start, zz, a if k == 0 else 0, b))
        start = start + a + b

    def place(n):
        base, zz, lo, b = parts[0]
        step = 0
        for k in range(1, 8):
            at_k = n >= parts[k][0]
            base = jnp.where(at_k, parts[k][0], base)
            zz = jnp.where(at_k, parts[k][1], zz)
            lo = jnp.where(at_k, parts[k][2], lo)
            b = jnp.where(at_k, parts[k][3], b)
            step = jnp.where(at_k, (k + 1) // 2, step)
        i = n - base
        is_b = ((i >= lo) & (i < lo + b)).astype(jnp.int32)
        s = 4 * zz + i - jnp.where(is_b == 1, lo, jnp.where(i < lo, 0, b))
        first = is_b * (4 * zm + 2) + (1 - is_b) * (4 * z)
        return (is_b, s, first, is_b * 8 + zz), step

    def stage1(slot, unit):
        is_b, s, first, _ = unit
        kv = kv_ref[s].reshape(SEG, 128)
        for r in range(0, 512, RC):
            b = first + r // 256
            idx = (s >= b).astype(jnp.int32) + (s > b).astype(jnp.int32)
            q = q_ref[pl.ds(pl.multiple_of(is_b * 512, 512) + r, RC), :]
            sc = lax.dot_general(q, kv, (((1,), (1,)), ((), ())), preferred_element_type=jnp.float32)
            sc = sc + mask_ref[idx, pl.ds(r % 256, RC), :]
            l = jnp.log2(1.0 + jnp.exp2(jnp.minimum(sc, 126.0)))
            sp = jnp.maximum(l, sc)
            sp_ref[slot, pl.ds(r, RC), :] = sp.astype(jnp.bfloat16)
            ls_ref[slot, pl.ds(r, RC), :] = sc - sp

    def stage2(slot):
        for r in range(0, 512, RC):
            sp = sp_ref[slot, pl.ds(r, RC), :]
            lo = jnp.dot(sp, tri_ref[:, 0:256], preferred_element_type=jnp.float32)
            hi = jnp.dot(sp[:, 256:], tri_ref[256:, 256:], preferred_element_type=jnp.float32)
            w_ref[slot, pl.ds(r, RC), 0:256] = jnp.exp2(ls_ref[slot, pl.ds(r, RC), 0:256] + lo).astype(jnp.bfloat16)
            w_ref[slot, pl.ds(r, RC), 256:512] = jnp.exp2(ls_ref[slot, pl.ds(r, RC), 256:512] + hi).astype(jnp.bfloat16)
            keep = lo[:, 0:1] - sp[:, 0:1].astype(jnp.float32)
            f_ref[slot, pl.ds(r, RC), :] = jnp.exp2(jnp.broadcast_to(keep, (RC, 128)))

    def stage3(slot, unit):
        _, s, _, at = unit
        kv = kv_ref[s].reshape(SEG, 128)
        for r in range(0, 512, RC):
            rows = pl.ds(r, RC)
            pv = jnp.dot(w_ref[slot, rows, :], kv, preferred_element_type=jnp.float32)
            f = f_ref[slot, rows, :]
            acc_ref[at, rows, :] = acc_ref[at, rows, :] * f + pv
            fac_ref[at, rows, :] = fac_ref[at, rows, :] * f

    u0, _ = place(0)
    u1, step = place(1)
    done, sib_done = arrive(-1, step, 7, 0)
    stage1(0, u0)
    stage2(0)
    stage1(1, u1)
    take_q(2)
    take_q(3)

    def body(i, carry):
        done, sib_done, ua, ub = carry
        uc, _ = place(2 * i + 2)
        ud, step = place(2 * i + 3)
        done, sib_done = arrive(i, step, done, sib_done)
        stage3(0, ua)
        stage2(1)
        stage1(0, uc)
        stage3(1, ub)
        stage2(0)
        stage1(1, ud)
        return done, sib_done, uc, ud

    done, sib_done, ua, ub = lax.fori_loop(0, (N_UNITS - 2) // 2, body, (done, sib_done, u0, u1))
    arrive(N_UNITS, 4, done, sib_done)
    stage3(0, ua)
    stage2(1)
    stage3(1, ub)


MESH = pl.DeviceIdType.MESH


def kernel(
    tok_hbm, wq_hbm, wk_hbm, wv_hbm, bias_hbm, wo_hbm, o_ref,
    tok, wq, wk, wv, bias, wo, qs, kvs, qp, q, kv, ob, at, obuf,
    mask_ref, tri_ref, sp_ref, ls_ref, w_ref, f_ref, acc_ref, fac_ref,
    out_s, loc, own_s, ownq_s, tok_s, tok_r, w_s, w_r, wo_s, wo_r, wos_s, wos_r,
    q_s, q_r, ya_s, ya_r, zr_s, zr_r, zl_s, zl_r, sib_s, sib_r, ex_s, ex_r,
):
    sp, tp = lax.axis_index("sp"), lax.axis_index("tp")
    z, y, x, c = sp // 4, sp % 4, tp // 2, tp % 2
    zm = 7 - z

    def dev(xx, yy, zz, cc):
        return (4 * zz + yy, 2 * xx + cc)

    def remote(src, dst, s, r, to):
        return pltpu.make_async_remote_copy(
            src_ref=src, dst_ref=dst, send_sem=s, recv_sem=r, device_id=to, device_id_type=MESH
        )

    sib = dev(x, y, z, 1 - c)
    right, left = dev(x, y, (z + 1) % 8, c), dev(x, y, (z + 7) % 8, c)

    locals_ = [
        pltpu.make_async_copy(a, b, loc.at[i])
        for i, (a, b) in enumerate(
            [(tok_hbm, tok.at[x]), (wq_hbm, wq.at[c]), (wk_hbm, wk.at[c]), (wv_hbm, wv.at[c]),
             (bias_hbm, bias.at[c]), (wo_hbm, wo.at[tp])]
        )
    ]
    for cp in locals_:
        cp.start()

    barrier = pltpu.get_barrier_semaphore()
    for dx in range(4):
        for dy in range(4):
            if dx or dy:
                pl.semaphore_signal(barrier, inc=1, device_id=dev((x + dx) % 4, (y + dy) % 4, z, c), device_id_type=MESH)
            pl.semaphore_signal(barrier, inc=1, device_id=dev((x + dx) % 4, (y + dy) % 4, zm, c), device_id_type=MESH)
    for to in (sib, right, left):
        pl.semaphore_signal(barrier, inc=1, device_id=to, device_id_type=MESH)
    pl.semaphore_wait(barrier, 34)

    x_right, x_left = dev((x + 1) % 4, y, z, c), dev((x + 3) % 4, y, z, c)
    around = (x, (x + 3) % 4, (x + 1) % 4, (x + 2) % 4)
    halves = (pl.ds(0, 32), pl.ds(32, 32))
    sends = []

    def go(cp):
        cp.start()
        sends.append(cp)

    for i in range(2):
        go(remote(tok_hbm.at[halves[i]], tok.at[x, halves[i]], tok_s.at[i], tok_r.at[2 + i], x_right))
        go(remote(tok_hbm.at[halves[1 - i]], tok.at[x, halves[1 - i]], tok_s.at[3 - i], tok_r.at[5 - i], x_left))
    shared = [(wq_hbm, wq), (wk_hbm, wk), (wv_hbm, wv), (bias_hbm, bias)]
    for i, (a, b) in enumerate(shared):
        go(remote(a, b.at[c], w_s.at[i], w_r.at[i], sib))

    acc_ref[...] = jnp.zeros_like(acc_ref)
    fac_ref[...] = jnp.ones_like(fac_ref)
    for i, (a, b) in enumerate(shared):
        remote(a, b.at[1 - c], w_s.at[i], w_r.at[i], sib).wait_recv()
    for cp in locals_:
        cp.wait()

    def tok_landed(o, i):
        there = tok.at[around[o], halves[i]]
        remote(there, there, tok_s.at[0], tok_r.at[2 * o + i], sib).wait_recv()

    def tok_on(o, i):
        there = tok.at[around[o], halves[i]]
        go(remote(there, there, tok_s.at[3 + o], tok_r.at[6 + i], x_right if o == 1 else x_left))

    zq = jnp.where(y < 2, z, zm)

    def own_q(o):
        xb = around[o]

        @pl.when(y < 2)
        def _():
            pltpu.make_async_copy(qs.at[y, xb], qp.at[y, xb], ownq_s.at[o]).start()

        @pl.when(y >= 2)
        def _():
            remote(qs.at[y, xb], qp.at[y, xb], q_s.at[4 * o], q_r.at[4 * y + o], dev(x, y, zm, c)).start()

    def project(o):
        xb = around[o]
        rows = tok[xb]
        for cc in range(2):
            qq = jnp.dot(rows, wq[cc], preferred_element_type=jnp.float32) * (LOG2E / 8)
            kk = jnp.dot(rows, wk[cc], preferred_element_type=jnp.float32)
            vv = jnp.dot(rows, wv[cc], preferred_element_type=jnp.float32)
            for j in range(2):
                lanes = slice(64 * j, 64 * j + 64)
                kvs[2 * cc + j, xb] = jnp.concatenate([vv[:, lanes], kk[:, lanes]], axis=1).astype(jnp.bfloat16)
                qs[2 * cc + j, xb] = jnp.concatenate([qq[:32, lanes], qq[32:, lanes]], axis=1).astype(jnp.bfloat16)
        for d in (2, 1, 3):
            yp = (y + d) % 4
            go(remote(qs.at[yp, xb], qp.at[y, xb], q_s.at[4 * o + d], q_r.at[4 * y + o], dev(x, yp, zq, c)))
        own_q(o)
        for d in (2, 1, 3):
            yp = (y + d) % 4
            go(remote(kvs.at[yp, xb], kv.at[4 * z + y, xb, c], ya_s.at[4 * o + d], ya_r.at[4 * o + y], dev(x, yp, z, c)))
        pltpu.make_async_copy(kvs.at[y, xb], kv.at[4 * z + y, xb, c], own_s.at[o]).start()

    def piece(zz, o):
        return kv.at[pl.ds(4 * zz, 4), row_of(o), c]

    def row_of(o):
        if isinstance(o, int):
            return around[o]
        return (x + jnp.where(o == 0, 0, jnp.where(o == 1, 3, o - 1))) % 4

    def pass_on(zz, o):
        return remote(piece(zz, o), piece(zz, o), sib_s.at[4 * zz + o], sib_r.at[4 * zz + o], sib)

    def source(way, t):
        return (z + 8 - t) % 8 if way == 0 else (z + t) % 8

    def hop(way, t, o, landing=0):
        zz = source(way, t + landing)
        s, r = ((zr_s, zr_r), (zl_s, zl_r))[way]
        return remote(piece(zz, o), piece(zz, o), s.at[4 * t + o], r.at[4 * t + o], (right, left)[way])

    def start_z(o):
        for d in (1, 3, 2):
            ys = (y + d) % 4
            there = kv.at[4 * z + ys, around[o], c]
            remote(there, there, ya_s.at[0], ya_r.at[4 * o + ys], sib).wait_recv()
        pltpu.make_async_copy(kvs.at[y, around[o]], kv.at[4 * z + y, around[o], c], own_s.at[o]).wait()
        for way in range(2):
            go(hop(way, 0, o))
        go(pass_on(z, o))

    project(0)
    tok_landed(1, 0)
    tok_on(1, 0)
    tok_landed(2, 1)
    tok_on(2, 1)
    both = bias[y // 2]
    b2 = jnp.where(y % 2 == 0, both[:, 0:1], both[:, 1:2]) * LOG2E
    start_z(0)
    tok_landed(1, 1)
    project(1)
    tok_landed(2, 0)
    project(2)
    start_z(1)
    tok_landed(3, 0)
    tok_landed(3, 1)
    project(3)
    go(remote(wo_hbm, wo.at[tp], wo_s.at[0], wo_r.at[2], x_right))
    go(remote(wo_hbm, wo.at[tp], wo_s.at[1], wo_r.at[4], x_left))
    build_tables(b2, c, mask_ref, tri_ref)
    def take_q(j):
        @pl.when((y == j) & (y < 2))
        def _():
            for o in range(4):
                pltpu.make_async_copy(qs.at[y, 0], qp.at[y, 0], ownq_s.at[o]).wait()

        @pl.when((y != j) | (y >= 2))
        def _():
            for o in range(4):
                remote(qs.at[0, 0], qp.at[j, around[o]], q_s.at[0], q_r.at[4 * j + o], sib).wait_recv()
        for xb in range(4):
            low = qp[j, xb].astype(jnp.float32)
            nil = jnp.zeros((32, 64), jnp.float32)
            at_row = 256 * j + 64 * xb
            q[pl.ds(at_row, 32), :] = jnp.concatenate([nil, low[:, :64]], axis=1).astype(jnp.bfloat16)
            q[pl.ds(at_row + 32, 32), :] = jnp.concatenate([nil, low[:, 64:]], axis=1).astype(jnp.bfloat16)

    wo_half = (pl.ds(0, 64), pl.ds(64, 64))

    def wo_hop(o, i):
        there = wo.at[2 * around[o] + c, wo_half[i]]
        return remote(there, there, wo_s.at[1 + o], wo_r.at[6 + i], x_right if o == 1 else x_left)

    def wo_share(o):
        there = wo.at[2 * around[o] + c]
        return remote(there, there, wos_s.at[o], wos_r.at[o], sib)

    def event(e, carry):
        t, o = e // 4, e % 4
        for way in range(2):
            @pl.when((t < 4) | (o // 2 == way))
            def _():
                hop(way, t - 1, o, 1).wait_recv()

                @pl.when((t < 3) | ((t == 3) & (o // 2 == way)))
                def _():
                    hop(way, t, o).start()
                pass_on(source(way, t), o).start()
        return carry

    def sib_event(e, carry):
        t, o = e // 4, e % 4

        def wait_for(zz):
            there = kv.at[pl.ds(4 * zz, 4), row_of(o), 1 - c]
            remote(there, there, sib_s.at[0], sib_r.at[4 * zz + o], sib).wait_recv()

        wait_for(source(0, t))

        @pl.when((t > 0) & (t < 4))
        def _():
            wait_for(source(1, t))
        return carry

    start_z(2)
    event(4, 0)
    take_q(0)
    take_q(1)
    start_z(3)
    event(5, 0)
    event(6, 0)

    def arrive(n, step, done, sib_done):
        need = 4 * step + 4
        upto = jnp.maximum(need, jnp.minimum(20, 10 + n * 4 // 3))
        lax.fori_loop(done, upto, event, 0)
        done = jnp.maximum(done, upto)
        lax.fori_loop(sib_done, need, sib_event, 0)
        sib_done = jnp.maximum(sib_done, need)

        @pl.when(n == WO_ON)
        def _():
            for o in (1, 2):
                there = wo.at[2 * around[o] + c]
                remote(there, there, wo_s.at[0], wo_r.at[2 * o], sib).wait_recv()
                wo_hop(o, o - 1).start()

        @pl.when(n == WO_SHARE)
        def _():
            for i in range(2):
                there = wo.at[2 * around[3] + c, wo_half[i]]
                remote(there, there, wo_s.at[0], wo_r.at[6 + i], sib).wait_recv()
            for o in range(4):
                wo_share(o).start()
        return done, sib_done

    attend(z, arrive, take_q, q, kv, mask_ref, tri_ref, sp_ref, ls_ref, w_ref, f_ref, acc_ref, fac_ref)

    for b in (1, 0):
        for r in range(0, 512, 64):
            rows = pl.ds(r, 64)
            total = acc_ref[8 * b, rows, :]
            for zz in range(1, 8):
                total = total * fac_ref[8 * b + zz, rows, :] + acc_ref[8 * b + zz, rows, :]
            ob[pl.ds(256 * b + r // 2, 32), :] = jnp.concatenate([total[:32, :64], total[32:, :64]], axis=1).astype(
                jnp.bfloat16
            )
    hh = 4 * x + y
    exits = []
    for i in (2, 3, 0, 1):
        for d in (2, 1, 3, 0):
            xb = (x + d) % 4
            src = ob.at[pl.ds(128 * i + pl.multiple_of(32 * xb, 32), 32), :]
            cp = remote(src, at.at[hh], ex_s.at[4 * i + d], ex_r.at[hh], dev(xb, i, z if i < 2 else zm, c))
            if d == 0 and i < 2:
                @pl.when(y != i)
                def _():
                    cp.start()

                @pl.when(y == i)
                def _():
                    here = pltpu.make_async_copy(src, at.at[hh], loc.at[8])
                    here.start()
                    here.wait()
            else:
                cp.start()
                exits.append(cp)
    for o in range(4):
        there = wo.at[2 * around[o] + 1 - c]
        remote(there, there, wos_s.at[o], wos_r.at[o], sib).wait_recv()
    for cp in sends:
        cp.wait_send()
    for o in range(4):
        wo_share(o).wait_send()
    for o in (1, 2):
        wo_hop(o, o - 1).wait_send()
    for t in range(1, 5):
        for o in range(4):
            for way in range(2):
                if t < 4 or o // 2 == way:
                    if t < 3 or (t == 3 and o // 2 == way):
                        hop(way, t, o).wait_send()
                    pass_on(source(way, t), o).wait_send()

    @pl.when(y >= 2)
    def _():
        for o in range(4):
            remote(qs.at[y, 0], qp.at[y, 0], q_s.at[4 * o], q_r.at[0], dev(x, y, zm, c)).wait_send()

    for g in range(16):
        @pl.when((hh != g) | (y >= 2))
        def _():
            remote(ob.at[pl.ds(0, 32), :], at.at[g], ex_s.at[0], ex_r.at[g], sib).wait_recv()

    heads = [at[h].astype(jnp.float32) for h in range(16)]
    upper = jnp.concatenate([head[:, :64] for head in heads], axis=1)
    lower = jnp.concatenate([head[:, 64:] for head in heads], axis=1)
    every = jnp.concatenate([upper, lower], axis=0).astype(jnp.bfloat16)
    for n in range(0, 2048, 512):
        obuf[:, n : n + 512] = jnp.dot(
            every, wo[:, :, n : n + 512].reshape(1024, 512), preferred_element_type=jnp.float32
        ).astype(jnp.bfloat16)
        pltpu.make_async_copy(obuf.at[:, n : n + 512], o_ref.at[:, n : n + 512], out_s.at[n // 512]).start()

    for cp in exits:
        cp.wait_send()
    for i in range(2):
        @pl.when(y != i)
        def _():
            remote(ob.at[pl.ds(0, 32), :], at.at[hh], ex_s.at[4 * i], ex_r.at[hh], sib).wait_send()

    for n in range(0, 2048, 512):
        pltpu.make_async_copy(obuf.at[:, n : n + 512], o_ref.at[:, n : n + 512], out_s.at[n // 512]).wait()


def shards(tokens, w_query, w_key, w_value, head_bias, w_out):
    bf, f32 = jnp.bfloat16, jnp.float32
    dma = pltpu.SemaphoreType.DMA
    return pl.pallas_call(
        kernel,
        out_shape=jax.ShapeDtypeStruct((64, 2048), bf),
        in_specs=[pl.BlockSpec(memory_space=pl.ANY)] * 6,
        out_specs=pl.BlockSpec(memory_space=pl.ANY),
        scratch_shapes=[
            pltpu.VMEM((4, 64, 2048), bf),
            pltpu.VMEM((2, 2048, 128), bf),
            pltpu.VMEM((2, 2048, 128), bf),
            pltpu.VMEM((2, 2048, 128), bf),
            pltpu.VMEM((2, 1, 2), f32),
            pltpu.VMEM((8, 128, 2048), bf),
            pltpu.VMEM((4, 4, 32, 128), bf),
            pltpu.VMEM((4, 4, 64, 128), bf),
            pltpu.VMEM((4, 4, 32, 128), bf),
            pltpu.VMEM((1024, 128), bf),
            pltpu.VMEM((32, 4, 2, 64, 128), bf),
            pltpu.VMEM((512, 128), bf),
            pltpu.VMEM((16, 32, 128), bf),
            pltpu.VMEM((64, 2048), bf),
            pltpu.VMEM((3, 256, SEG), f32),
            pltpu.VMEM((SEG, SEG), bf),
            pltpu.VMEM((2, SEG, SEG), bf),
            pltpu.VMEM((2, SEG, SEG), f32),
            pltpu.VMEM((2, SEG, SEG), bf),
            pltpu.VMEM((2, SEG, 128), f32),
            pltpu.VMEM((16, SEG, 128), f32),
            pltpu.VMEM((16, SEG, 128), f32),
            dma((4,)), dma((9,)), dma((4,)), dma((4,)), dma((6,)), dma((8,)), dma((4,)), dma((4,)), dma((4,)), dma((8,)), dma((4,)),
            dma((4,)), dma((16,)), dma((16,)), dma((16,)), dma((16,)), dma((16,)), dma((16,)), dma((16,)), dma((16,)),
            dma((32,)), dma((32,)), dma((16,)), dma((16,)),
        ],
        compiler_params=pltpu.CompilerParams(
            vmem_limit_bytes=60 * 2**20, collective_id=0, has_side_effects=True
        ),
        name="layer",
    )(tokens, w_query, w_key, w_value, head_bias.reshape(1, 2), w_out)


def solution(mesh):
    placed = (P(("sp", "tp"), None), P(None, "tp"), P(None, "tp"), P(None, "tp"), P("tp"), P("tp", None))
    return jax.shard_map(
        shards, mesh=mesh, in_specs=placed, out_specs=P(("sp", "tp"), None), check_vma=False
    )
```

```python
import jax, jax.numpy as jnp
from jax import lax
from jax.sharding import PartitionSpec as P
from jax.experimental import pallas as pl
from jax.experimental.pallas import tpu as pltpu

LOG2E = 1.4426950408889634
SEG = 512
N_UNITS = 34
WO_ON, WO_SHARE = 8, 13
ORDER = (0, 7, 1, 6, 2, 5, 3, 4)
NEG = -1e30

def build_tables(bias2, c, mask_ref, tri_ref):
    rows = lax.broadcasted_iota(jnp.int32, (256, SEG), 0)
    cols = lax.broadcasted_iota(jnp.int32, (256, SEG), 1)
    qpos = (2 * (rows // 64) + c) * 64 + rows % 64
    mask_ref[0] = jnp.full((256, SEG), bias2, jnp.float32)
    mask_ref[1] = jnp.where(cols < qpos, bias2, NEG)
    mask_ref[2] = jnp.full((256, SEG), NEG, jnp.float32)
    j = lax.broadcasted_iota(jnp.int32, (SEG, SEG), 0)
    s = lax.broadcasted_iota(jnp.int32, (SEG, SEG), 1)
    tri_ref[...] = jnp.where(j > s, -1.0, 0.0).astype(jnp.bfloat16)

def attend(z, arrive, take_q, q_ref, kv_ref, mask_ref, tri_ref, sp_ref, ls_ref, w_ref, f_ref, acc_ref, fac_ref, RC=128):
    zm = 7 - z
    parts = []
    start = 0
    for k in range(8):
        zz = (z + ORDER[k]) % 8
        a = 4 * (zz < z).astype(jnp.int32) + 2 * (zz == z).astype(jnp.int32)
        b = 4 * (zz <= zm).astype(jnp.int32)
        parts.append((start, zz, a if k == 0 else 0, b))
        start = start + a + b

    def place(n):
        base, zz, lo, b = parts[0]
        step = 0
        for k in range(1, 8):
            at_k = n >= parts[k][0]
            base = jnp.where(at_k, parts[k][0], base)
            zz = jnp.where(at_k, parts[k][1], zz)
            lo = jnp.where(at_k, parts[k][2], lo)
            b = jnp.where(at_k, parts[k][3], b)
            step = jnp.where(at_k, (k + 1) // 2, step)
        i = n - base
        is_b = ((i >= lo) & (i < lo + b)).astype(jnp.int32)
        s = 4 * zz + i - jnp.where(is_b == 1, lo, jnp.where(i < lo, 0, b))
        first = is_b * (4 * zm + 2) + (1 - is_b) * (4 * z)
        return (is_b, s, first, is_b * 8 + zz), step

    def stage1(slot, unit):
        is_b, s, first, _ = unit
        kv = kv_ref[s].reshape(SEG, 128)
        for r in range(0, 512, RC):
            b = first + r // 256
            idx = (s >= b).astype(jnp.int32) + (s > b).astype(jnp.int32)
            q = q_ref[pl.ds(pl.multiple_of(is_b * 512, 512) + r, RC), :]
            sc = lax.dot_general(q, kv, (((1,), (1,)), ((), ())), preferred_element_type=jnp.float32)
            sc = sc + mask_ref[idx, pl.ds(r % 256, RC), :]
            l = jnp.log2(1.0 + jnp.exp2(jnp.minimum(sc, 126.0)))
            sp = jnp.maximum(l, sc)
            sp_ref[slot, pl.ds(r, RC), :] = sp.astype(jnp.bfloat16)
            ls_ref[slot, pl.ds(r, RC), :] = sc - sp

    def stage2(slot):
        for r in range(0, 512, RC):
            sp = sp_ref[slot, pl.ds(r, RC), :]
            lo = jnp.dot(sp, tri_ref[:, 0:256], preferred_element_type=jnp.float32)
            hi = jnp.dot(sp[:, 256:], tri_ref[256:, 256:], preferred_element_type=jnp.float32)
            w_ref[slot, pl.ds(r, RC), 0:256] = jnp.exp2(ls_ref[slot, pl.ds(r, RC), 0:256] + lo).astype(jnp.bfloat16)
            w_ref[slot, pl.ds(r, RC), 256:512] = jnp.exp2(ls_ref[slot, pl.ds(r, RC), 256:512] + hi).astype(jnp.bfloat16)
            keep = lo[:, 0:1] - sp[:, 0:1].astype(jnp.float32)
            f_ref[slot, pl.ds(r, RC), :] = jnp.exp2(jnp.broadcast_to(keep, (RC, 128)))

    def stage3(slot, unit):
        _, s, _, at = unit
        kv = kv_ref[s].reshape(SEG, 128)
        for r in range(0, 512, RC):
            rows = pl.ds(r, RC)
            pv = jnp.dot(w_ref[slot, rows, :], kv, preferred_element_type=jnp.float32)
            f = f_ref[slot, rows, :]
            acc_ref[at, rows, :] = acc_ref[at, rows, :] * f + pv
            fac_ref[at, rows, :] = fac_ref[at, rows, :] * f

    u0, _ = place(0)
    u1, step = place(1)
    done, sib_done = arrive(-1, step, 7, 0)
    stage1(0, u0)
    stage2(0)
    stage1(1, u1)
    take_q(2)
    take_q(3)

    def body(i, carry):
        done, sib_done, ua, ub = carry
        uc, _ = place(2 * i + 2)
        ud, step = place(2 * i + 3)
        done, sib_done = arrive(i, step, done, sib_done)
        stage3(0, ua)
        stage2(1)
        stage1(0, uc)
        stage3(1, ub)
        stage2(0)
        stage1(1, ud)
        return done, sib_done, uc, ud

    done, sib_done, ua, ub = lax.fori_loop(0, (N_UNITS - 2) // 2, body, (done, sib_done, u0, u1))
    arrive(N_UNITS, 4, done, sib_done)
    stage3(0, ua)
    stage2(1)
    stage3(1, ub)


MESH = pl.DeviceIdType.MESH


def kernel(
    tok_hbm, wq_hbm, wk_hbm, wv_hbm, bias_hbm, wo_hbm, o_ref,
    tok, wq, wk, wv, bias, wo, qs, kvs, qp, q, kv, ob, at, obuf,
    mask_ref, tri_ref, sp_ref, ls_ref, w_ref, f_ref, acc_ref, fac_ref,
    out_s, loc, own_s, ownq_s, tok_s, tok_r, w_s, w_r, wo_s, wo_r, wos_s, wos_r,
    q_s, q_r, ya_s, ya_r, zr_s, zr_r, zl_s, zl_r, sib_s, sib_r, ex_s, ex_r,
):
    sp, tp = lax.axis_index("sp"), lax.axis_index("tp")
    z, y, x, c = sp // 4, sp % 4, tp // 2, tp % 2
    zm = 7 - z

    def dev(xx, yy, zz, cc):
        return (4 * zz + yy, 2 * xx + cc)

    def remote(src, dst, s, r, to):
        return pltpu.make_async_remote_copy(
            src_ref=src, dst_ref=dst, send_sem=s, recv_sem=r, device_id=to, device_id_type=MESH
        )

    sib = dev(x, y, z, 1 - c)
    right, left = dev(x, y, (z + 1) % 8, c), dev(x, y, (z + 7) % 8, c)

    locals_ = [
        pltpu.make_async_copy(a, b, loc.at[i])
        for i, (a, b) in enumerate(
            [(tok_hbm, tok.at[x]), (wq_hbm, wq.at[c]), (wk_hbm, wk.at[c]), (wv_hbm, wv.at[c]),
             (bias_hbm, bias.at[c]), (wo_hbm, wo.at[tp])]
        )
    ]
    for cp in locals_:
        cp.start()

    barrier = pltpu.get_barrier_semaphore()
    for dx in range(4):
        for dy in range(4):
            if dx or dy:
                pl.semaphore_signal(barrier, inc=1, device_id=dev((x + dx) % 4, (y + dy) % 4, z, c), device_id_type=MESH)
            pl.semaphore_signal(barrier, inc=1, device_id=dev((x + dx) % 4, (y + dy) % 4, zm, c), device_id_type=MESH)
    for to in (sib, right, left):
        pl.semaphore_signal(barrier, inc=1, device_id=to, device_id_type=MESH)
    pl.semaphore_wait(barrier, 34)

    x_right, x_left = dev((x + 1) % 4, y, z, c), dev((x + 3) % 4, y, z, c)
    around = (x, (x + 3) % 4, (x + 1) % 4, (x + 2) % 4)
    halves = (pl.ds(0, 32), pl.ds(32, 32))
    sends = []

    def go(cp):
        cp.start()
        sends.append(cp)

    for i in range(2):
        go(remote(tok_hbm.at[halves[i]], tok.at[x, halves[i]], tok_s.at[i], tok_r.at[2 + i], x_right))
        go(remote(tok_hbm.at[halves[1 - i]], tok.at[x, halves[1 - i]], tok_s.at[3 - i], tok_r.at[5 - i], x_left))
    shared = [(wq_hbm, wq), (wk_hbm, wk), (wv_hbm, wv), (bias_hbm, bias)]
    for i, (a, b) in enumerate(shared):
        go(remote(a, b.at[c], w_s.at[i], w_r.at[i], sib))

    acc_ref[...] = jnp.zeros_like(acc_ref)
    fac_ref[...] = jnp.ones_like(fac_ref)
    for i, (a, b) in enumerate(shared):
        remote(a, b.at[1 - c], w_s.at[i], w_r.at[i], sib).wait_recv()
    for cp in locals_:
        cp.wait()

    def tok_landed(o, i):
        there = tok.at[around[o], halves[i]]
        remote(there, there, tok_s.at[0], tok_r.at[2 * o + i], sib).wait_recv()

    def tok_on(o, i):
        there = tok.at[around[o], halves[i]]
        go(remote(there, there, tok_s.at[3 + o], tok_r.at[6 + i], x_right if o == 1 else x_left))

    zq = jnp.where(y < 2, z, zm)

    def own_q(o):
        xb = around[o]

        @pl.when(y < 2)
        def _():
            pltpu.make_async_copy(qs.at[y, xb], qp.at[y, xb], ownq_s.at[o]).start()

        @pl.when(y >= 2)
        def _():
            remote(qs.at[y, xb], qp.at[y, xb], q_s.at[4 * o], q_r.at[4 * y + o], dev(x, y, zm, c)).start()

    def project(o):
        xb = around[o]
        rows = tok[xb]
        for cc in range(2):
            qq = jnp.dot(rows, wq[cc], preferred_element_type=jnp.float32) * (LOG2E / 8)
            kk = jnp.dot(rows, wk[cc], preferred_element_type=jnp.float32)
            vv = jnp.dot(rows, wv[cc], preferred_element_type=jnp.float32)
            for j in range(2):
                lanes = slice(64 * j, 64 * j + 64)
                kvs[2 * cc + j, xb] = jnp.concatenate([vv[:, lanes], kk[:, lanes]], axis=1).astype(jnp.bfloat16)
                qs[2 * cc + j, xb] = jnp.concatenate([qq[:32, lanes], qq[32:, lanes]], axis=1).astype(jnp.bfloat16)
        for d in (2, 1, 3):
            yp = (y + d) % 4
            go(remote(qs.at[yp, xb], qp.at[y, xb], q_s.at[4 * o + d], q_r.at[4 * y + o], dev(x, yp, zq, c)))
        own_q(o)
        for d in (2, 1, 3):
            yp = (y + d) % 4
            go(remote(kvs.at[yp, xb], kv.at[4 * z + y, xb, c], ya_s.at[4 * o + d], ya_r.at[4 * o + y], dev(x, yp, z, c)))
        pltpu.make_async_copy(kvs.at[y, xb], kv.at[4 * z + y, xb, c], own_s.at[o]).start()

    def piece(zz, o):
        return kv.at[pl.ds(4 * zz, 4), row_of(o), c]

    def row_of(o):
        if isinstance(o, int):
            return around[o]
        return (x + jnp.where(o == 0, 0, jnp.where(o == 1, 3, o - 1))) % 4

    def pass_on(zz, o):
        return remote(piece(zz, o), piece(zz, o), sib_s.at[4 * zz + o], sib_r.at[4 * zz + o], sib)

    def source(way, t):
        return (z + 8 - t) % 8 if way == 0 else (z + t) % 8

    def hop(way, t, o, landing=0):
        zz = source(way, t + landing)
        s, r = ((zr_s, zr_r), (zl_s, zl_r))[way]
        return remote(piece(zz, o), piece(zz, o), s.at[4 * t + o], r.at[4 * t + o], (right, left)[way])

    def start_z(o):
        for d in (1, 3, 2):
            ys = (y + d) % 4
            there = kv.at[4 * z + ys, around[o], c]
            remote(there, there, ya_s.at[0], ya_r.at[4 * o + ys], sib).wait_recv()
        pltpu.make_async_copy(kvs.at[y, around[o]], kv.at[4 * z + y, around[o], c], own_s.at[o]).wait()
        for way in range(2):
            go(hop(way, 0, o))
        go(pass_on(z, o))

    project(0)
    tok_landed(1, 0)
    tok_on(1, 0)
    tok_landed(2, 1)
    tok_on(2, 1)
    both = bias[y // 2]
    b2 = jnp.where(y % 2 == 0, both[:, 0:1], both[:, 1:2]) * LOG2E
    start_z(0)
    tok_landed(1, 1)
    project(1)
    tok_landed(2, 0)
    project(2)
    start_z(1)
    tok_landed(3, 0)
    tok_landed(3, 1)
    project(3)
    go(remote(wo_hbm, wo.at[tp], wo_s.at[0], wo_r.at[2], x_right))
    go(remote(wo_hbm, wo.at[tp], wo_s.at[1], wo_r.at[4], x_left))
    build_tables(b2, c, mask_ref, tri_ref)
    def take_q(j):
        @pl.when((y == j) & (y < 2))
        def _():
            for o in range(4):
                pltpu.make_async_copy(qs.at[y, 0], qp.at[y, 0], ownq_s.at[o]).wait()

        @pl.when((y != j) | (y >= 2))
        def _():
            for o in range(4):
                remote(qs.at[0, 0], qp.at[j, around[o]], q_s.at[0], q_r.at[4 * j + o], sib).wait_recv()
        for xb in range(4):
            low = qp[j, xb].astype(jnp.float32)
            nil = jnp.zeros((32, 64), jnp.float32)
            at_row = 256 * j + 64 * xb
            q[pl.ds(at_row, 32), :] = jnp.concatenate([nil, low[:, :64]], axis=1).astype(jnp.bfloat16)
            q[pl.ds(at_row + 32, 32), :] = jnp.concatenate([nil, low[:, 64:]], axis=1).astype(jnp.bfloat16)

    wo_half = (pl.ds(0, 64), pl.ds(64, 64))

    def wo_hop(o, i):
        there = wo.at[2 * around[o] + c, wo_half[i]]
        return remote(there, there, wo_s.at[1 + o], wo_r.at[6 + i], x_right if o == 1 else x_left)

    def wo_share(o):
        there = wo.at[2 * around[o] + c]
        return remote(there, there, wos_s.at[o], wos_r.at[o], sib)

    def event(e, carry):
        t, o = e // 4, e % 4
        for way in range(2):
            @pl.when((t < 4) | (o // 2 == way))
            def _():
                hop(way, t - 1, o, 1).wait_recv()

                @pl.when((t < 3) | ((t == 3) & (o // 2 == way)))
                def _():
                    hop(way, t, o).start()
                pass_on(source(way, t), o).start()
        return carry

    def sib_event(e, carry):
        t, o = e // 4, e % 4

        def wait_for(zz):
            there = kv.at[pl.ds(4 * zz, 4), row_of(o), 1 - c]
            remote(there, there, sib_s.at[0], sib_r.at[4 * zz + o], sib).wait_recv()

        wait_for(source(0, t))

        @pl.when((t > 0) & (t < 4))
        def _():
            wait_for(source(1, t))
        return carry

    start_z(2)
    event(4, 0)
    take_q(0)
    take_q(1)
    start_z(3)
    event(5, 0)
    event(6, 0)

    def arrive(n, step, done, sib_done):
        need = 4 * step + 4
        upto = jnp.maximum(need, jnp.minimum(20, 10 + n * 4 // 3))
        lax.fori_loop(done, upto, event, 0)
        done = jnp.maximum(done, upto)
        lax.fori_loop(sib_done, need, sib_event, 0)
        sib_done = jnp.maximum(sib_done, need)

        @pl.when(n == WO_ON)
        def _():
            for o in (1, 2):
                there = wo.at[2 * around[o] + c]
                remote(there, there, wo_s.at[0], wo_r.at[2 * o], sib).wait_recv()
                wo_hop(o, o - 1).start()

        @pl.when(n == WO_SHARE)
        def _():
            for i in range(2):
                there = wo.at[2 * around[3] + c, wo_half[i]]
                remote(there, there, wo_s.at[0], wo_r.at[6 + i], sib).wait_recv()
            for o in range(4):
                wo_share(o).start()
        return done, sib_done

    attend(z, arrive, take_q, q, kv, mask_ref, tri_ref, sp_ref, ls_ref, w_ref, f_ref, acc_ref, fac_ref)

    for b in (1, 0):
        for r in range(0, 512, 64):
            rows = pl.ds(r, 64)
            total = acc_ref[8 * b, rows, :]
            for zz in range(1, 8):
                total = total * fac_ref[8 * b + zz, rows, :] + acc_ref[8 * b + zz, rows, :]
            ob[pl.ds(256 * b + r // 2, 32), :] = jnp.concatenate([total[:32, :64], total[32:, :64]], axis=1).astype(
                jnp.bfloat16
            )
    hh = 4 * x + y
    exits = []
    for i in (2, 3, 0, 1):
        for d in (2, 1, 3, 0):
            xb = (x + d) % 4
            src = ob.at[pl.ds(128 * i + pl.multiple_of(32 * xb, 32), 32), :]
            cp = remote(src, at.at[hh], ex_s.at[4 * i + d], ex_r.at[hh], dev(xb, i, z if i < 2 else zm, c))
            if d == 0 and i < 2:
                @pl.when(y != i)
                def _():
                    cp.start()

                @pl.when(y == i)
                def _():
                    here = pltpu.make_async_copy(src, at.at[hh], loc.at[8])
                    here.start()
                    here.wait()
            else:
                cp.start()
                exits.append(cp)
    for o in range(4):
        there = wo.at[2 * around[o] + 1 - c]
        remote(there, there, wos_s.at[o], wos_r.at[o], sib).wait_recv()
    for cp in sends:
        cp.wait_send()
    for o in range(4):
        wo_share(o).wait_send()
    for o in (1, 2):
        wo_hop(o, o - 1).wait_send()
    for t in range(1, 5):
        for o in range(4):
            for way in range(2):
                if t < 4 or o // 2 == way:
                    if t < 3 or (t == 3 and o // 2 == way):
                        hop(way, t, o).wait_send()
                    pass_on(source(way, t), o).wait_send()

    @pl.when(y >= 2)
    def _():
        for o in range(4):
            remote(qs.at[y, 0], qp.at[y, 0], q_s.at[4 * o], q_r.at[0], dev(x, y, zm, c)).wait_send()

    for g in range(16):
        @pl.when((hh != g) | (y >= 2))
        def _():
            remote(ob.at[pl.ds(0, 32), :], at.at[g], ex_s.at[0], ex_r.at[g], sib).wait_recv()

    heads = [at[h].astype(jnp.float32) for h in range(16)]
    upper = jnp.concatenate([head[:, :64] for head in heads], axis=1)
    lower = jnp.concatenate([head[:, 64:] for head in heads], axis=1)
    every = jnp.concatenate([upper, lower], axis=0).astype(jnp.bfloat16)
    for n in range(0, 2048, 512):
        obuf[:, n : n + 512] = jnp.dot(
            every, wo[:, :, n : n + 512].reshape(1024, 512), preferred_element_type=jnp.float32
        ).astype(jnp.bfloat16)
        pltpu.make_async_copy(obuf.at[:, n : n + 512], o_ref.at[:, n : n + 512], out_s.at[n // 512]).start()

    for cp in exits:
        cp.wait_send()
    for i in range(2):
        @pl.when(y != i)
        def _():
            remote(ob.at[pl.ds(0, 32), :], at.at[hh], ex_s.at[4 * i], ex_r.at[hh], sib).wait_send()

    for n in range(0, 2048, 512):
        pltpu.make_async_copy(obuf.at[:, n : n + 512], o_ref.at[:, n : n + 512], out_s.at[n // 512]).wait()


def shards(tokens, w_query, w_key, w_value, head_bias, w_out):
    bf, f32 = jnp.bfloat16, jnp.float32
    dma = pltpu.SemaphoreType.DMA
    return pl.pallas_call(
        kernel,
        out_shape=jax.ShapeDtypeStruct((64, 2048), bf),
        in_specs=[pl.BlockSpec(memory_space=pl.ANY)] * 6,
        out_specs=pl.BlockSpec(memory_space=pl.ANY),
        scratch_shapes=[
            pltpu.VMEM((4, 64, 2048), bf),
            pltpu.VMEM((2, 2048, 128), bf),
            pltpu.VMEM((2, 2048, 128), bf),
            pltpu.VMEM((2, 2048, 128), bf),
            pltpu.VMEM((2, 1, 2), f32),
            pltpu.VMEM((8, 128, 2048), bf),
            pltpu.VMEM((4, 4, 32, 128), bf),
            pltpu.VMEM((4, 4, 64, 128), bf),
            pltpu.VMEM((4, 4, 32, 128), bf),
            pltpu.VMEM((1024, 128), bf),
            pltpu.VMEM((32, 4, 2, 64, 128), bf),
            pltpu.VMEM((512, 128), bf),
            pltpu.VMEM((16, 32, 128), bf),
            pltpu.VMEM((64, 2048), bf),
            pltpu.VMEM((3, 256, SEG), f32),
            pltpu.VMEM((SEG, SEG), bf),
            pltpu.VMEM((2, SEG, SEG), bf),
            pltpu.VMEM((2, SEG, SEG), f32),
            pltpu.VMEM((2, SEG, SEG), bf),
            pltpu.VMEM((2, SEG, 128), f32),
            pltpu.VMEM((16, SEG, 128), f32),
            pltpu.VMEM((16, SEG, 128), f32),
            dma((4,)), dma((9,)), dma((4,)), dma((4,)), dma((6,)), dma((8,)), dma((4,)), dma((4,)), dma((4,)), dma((8,)), dma((4,)),
            dma((4,)), dma((16,)), dma((16,)), dma((16,)), dma((16,)), dma((16,)), dma((16,)), dma((16,)), dma((16,)),
            dma((32,)), dma((32,)), dma((16,)), dma((16,)),
        ],
        compiler_params=pltpu.CompilerParams(
            vmem_limit_bytes=36 * 2**20, collective_id=0, has_side_effects=True
        ),
        name="layer",
    )(tokens, w_query, w_key, w_value, head_bias.reshape(1, 2), w_out)


def solution(mesh):
    placed = (P(("sp", "tp"), None), P(None, "tp"), P(None, "tp"), P(None, "tp"), P("tp"), P("tp", None))
    return jax.shard_map(
        shards, mesh=mesh, in_specs=placed, out_specs=P(("sp", "tp"), None), check_vma=False
    )
```
